256 devices in a mesh: sp: 64 (over z, x, core), tp: 4 (over y).
Axes of the slice: x: 4, y: 4, z: 8, core: 2. Of those that a mesh axis runs over, the one named last changes fastest.
Arguments:
- residual: bfloat16 [24576, 2048], P(('sp', 'tp')), may hold values from -6 to 6
- queries: bfloat16 [24576, 1024], P('sp', 'tp'), may hold values from -2.5 to 2.5
- keys: bfloat16 [24576, 256], P('sp', 'tp'), may hold values from -2.5 to 2.5
- values: bfloat16 [24576, 256], P('sp', 'tp'), may hold values from -6 to 6
- documents: int32 [24576], P('sp'), may hold values from 0 to 32, never falling along the last dimension, each value on 1 to 1536 neighbouring positions
- sink: float32 [16], P('tp'), may hold values from 3 to 7
- out_weight: bfloat16 [1024, 2048], replicated, may hold values from -0.1875 to 0.1875
- mix_gain: float32 [2048], replicated, may hold values from 0.1 to 1.9
- ffn_gain: float32 [2048], replicated, may hold values from 0.1 to 1.9
- out_gain: float32 [2048], replicated, may hold values from 0.1 to 1.9
- routes: int32 [24576, 4], P(('sp', 'tp')), may hold values from 0 to 63, all different within a row; in each aligned block of 96 rows (0 to 95, 96 to 191, ...) at most 8 rows name the same one
- route_logits: float32 [24576, 4], P(('sp', 'tp')), may hold values from -4 to 4
- gate_weight: bfloat16 [64, 2048, 2048], P('sp', None, 'tp'), may hold values from -1.41421356 to 1.41421356
- up_weight: bfloat16 [64, 2048, 2048], P('sp', None, 'tp'), may hold values from -1.41421356 to 1.41421356
- down_weight: bfloat16 [64, 2048, 2048], P('sp', 'tp'), may hold values from -0.125 to 0.125
Outputs:
- mixed: bfloat16 [24576, 2048], P(('sp', 'tp'))
The draws below stay inside these ranges and needn't reach their ends.
Inputs may be any that keep to these rules, and one draw needn't show every extreme that they name: `routes`: each row names 4 different experts. In each aligned block of rows held by one device, no expert is named by more than 8 rows, a bound that some block reaches. `documents`: document numbers never fall along the positions; each document has 1 to 1536 positions, and one has exactly 1536.
All inputs are finite; a program needn't handle non-finite values.
Results may differ from the reference program's by a relative error of at most 0.017.
Values may be sent and summed in bfloat16 or wider, within the bound.
A program may use at most 128 MiB of HBM per device.

```python
import math
import jax
import jax.numpy as jnp
import numpy as np
from jax import lax

D = 2048
QH = 16
KVH = 4
HD = 64
FF = 2048
TOPK = 4
W = 128
TOK_DEV = 384
TOKENS = 24576
EXPERTS = 64
CAP = 8
DOCS = 33
DOC_MOST = 1536
N_TP = 4


def column_scaled(key):
    base_key, scale_key = jax.random.split(key)
    shape = (EXPERTS, D, FF)
    base = jnp.clip(jax.random.normal(base_key, shape, jnp.float32), -4.0, 4.0)
    column_scale = jnp.exp(jax.random.uniform(scale_key, (EXPERTS, 1, FF), jnp.float32, 0.0, 2.3025851))
    return (base * column_scale * D ** (-0.5)).astype(jnp.bfloat16)


def draw_gate_weight(key, part):
    return column_scaled(jax.random.fold_in(key, 11))


def draw_up_weight(key, part):
    return column_scaled(jax.random.fold_in(key, 23))


def block_scale(own_key, dims, cuts, smallest, high):
    factor_of, own = 1.0, jax.random.fold_in(own_key, 6)
    for dim, parts in cuts:
        heights = jnp.exp(jax.random.uniform(jax.random.fold_in(own, dim), (parts,), jnp.float32, smallest / len(cuts), high / len(cuts)))
        factor_of = factor_of * jnp.repeat(heights, dims[dim] // parts).reshape([-1 if axis == dim else 1 for axis in range(len(dims))])
    return factor_of


def profile(count, total, limit, skew):
    weights = [(1 << 20) // math.isqrt(grade ** skew) + 1 for grade in range(2, count + 1)]
    rest, given = total - limit - (count - 1), [1] * (count - 1)
    while rest > 0:
        free = [i for i in range(count - 1) if given[i] < limit]
        mass, remaining = sum([weights[i] for i in free]), rest
        for i in free:
            addition = min(limit - given[i], max(1, remaining * weights[i] // mass), rest)
            given[i] = given[i] + addition
            rest = rest - addition
    return np.array([limit] + given)


def uneven(own_key, amount, total, limit, skew):
    if amount == 2:
        one = jax.random.randint(own_key, (), max(1, total - limit), min(limit, total - 1) + 1)
        return jnp.stack([one, total - one])
    tallies = jnp.asarray(profile(amount, total, limit, skew), jnp.int32)
    couples = (amount - 1) // 2
    giver, taker = tallies[1:1 + 2 * couples:2], tallies[2:2 + 2 * couples:2]
    margin = jnp.minimum(giver - 1, limit - taker)
    shifted = jax.random.randint(jax.random.fold_in(own_key, 1), (couples,), 0, 1 << 20) % (margin + 1)
    tallies = tallies.at[1:1 + 2 * couples:2].set(giver - shifted).at[2:2 + 2 * couples:2].set(taker + shifted)
    return tallies[jax.random.permutation(jax.random.fold_in(own_key, 2), amount)]


def deal_out(stream_key, own, number, rows, count, top, bound, skew):
    sequence = jax.random.permutation(stream_key, count)
    packed, common = load_shares(count, rows * top, bound, skew, True), load_shares(count, rows * top, bound, skew, False)
    places = jnp.arange(count)

    def named(tallies, turn):
        used = int((tallies > 0).sum())
        fixed = max(1, used // 4)
        moved = fixed + (places - fixed + turn * (used - fixed)) % max(1, count - fixed)
        return jnp.zeros((count,), jnp.int32).at[sequence[jnp.where(places < fixed, places, moved)]].set(jnp.asarray(tallies, jnp.int32))

    tallies = jnp.where(number % 4 == 0, named(packed, number // 4), named(common, number - number // 4 - 1))
    mixed = jax.random.permutation(jax.random.fold_in(own, 3), count)
    giver, taker = mixed[0:count // 2 * 2:2], mixed[1:count // 2 * 2:2]
    slack = jnp.minimum(tallies[giver] - 1, bound - tallies[taker]) // 2
    slack = jnp.where((giver == sequence[0]) | (taker == sequence[0]) | (tallies[taker] == 0), 0, jnp.maximum(slack, 0))
    moved = jax.random.randint(jax.random.fold_in(own, 4), (count // 2,), 0, 1 << 20) % (slack + 1)
    tallies = tallies.at[giver].add(-moved).at[taker].add(moved)
    members = jnp.searchsorted(jnp.cumsum(tallies), jnp.arange(rows * top), side="right").astype(jnp.int32)
    listing = members.reshape(top, rows).T
    listing = listing[jax.random.permutation(jax.random.fold_in(own, 1), rows)]
    turn = jax.random.randint(jax.random.fold_in(own, 2), (rows, 1), 0, top)
    return jnp.take_along_axis(listing, (jnp.arange(top)[None, :] + turn) % top, axis=1)


def load_shares(number_of, total, limit, skew, full):
    weights = [(1 << 20) // math.isqrt(rank ** skew) + 1 for rank in range(1, number_of + 1)]
    largest = limit if full else min(limit, max(-(-total // number_of), total * weights[0] // sum(weights)))
    least = 1 if total - largest >= number_of - 1 else 0
    given, rest = [largest] + [least] * (number_of - 1), total - largest - least * (number_of - 1)
    while rest > 0:
        candidates = [i for i in range(1, number_of) if given[i] < largest] or [i for i in range(1, number_of) if given[i] < limit]
        mass, budget = sum([weights[i] for i in candidates]), rest
        for i in candidates:
            more = min(limit - given[i], max(1, budget * weights[i] // mass), rest)
            given[i] = given[i] + more
            rest = rest - more
    return np.array(given)


def noise(key, shape, width, most, shards=(), kind=jnp.bfloat16):
    array = jax.random.normal(key, shape, jnp.float32) * width
    if len(shards) > 0:
        array = block_scale(key, shape, shards, -0.22, 0.18) * array
    return jnp.clip(array, min=-most, max=most).astype(kind)


def setup_inputs(seed: int = 0) -> dict:
    splits = jax.random.split(jax.random.key(seed), 16)
    residual = noise(splits[0], (TOKENS, D), 1.0, 6.0, ((0, 256),))
    queries = noise(splits[1], (TOKENS, QH * HD), 1.0, 2.5, ((0, 64), (1, 4)))
    keys = noise(splits[2], (TOKENS, KVH * HD), 1.0, 2.5, ((0, 64), (1, 4)))
    values = noise(splits[3], (TOKENS, KVH * HD), 1.0, 6.0, ((0, 64), (1, 4)))
    documents = jnp.searchsorted(jnp.cumsum(uneven(splits[4], DOCS, TOKENS, DOC_MOST, 1)), jnp.arange(TOKENS), side="right").astype(jnp.int32)
    sink = jnp.clip(3.0 + 4.0 * jax.random.uniform(splits[5], (QH,), jnp.float32) ** block_scale(splits[5], (QH,), ((0, 4),), -0.2, 0.2), 3.0, 7.0)
    out_weight = noise(splits[6], (QH * HD, D), (QH * HD) ** -0.5, 0.1875)
    mix_gain = jnp.clip(1.0 + 0.18 * jax.random.normal(splits[7], (D,), jnp.float32), 0.1, 1.9)
    ffn_gain = jnp.clip(1.0 + 0.18 * jax.random.normal(splits[8], (D,), jnp.float32), 0.1, 1.9)
    out_gain = jnp.clip(1.0 + 0.18 * jax.random.normal(splits[9], (D,), jnp.float32), 0.1, 1.9)
    routes_keys = jax.random.split(jax.random.fold_in(splits[10], 1), TOKENS // (TOK_DEV // N_TP))
    routes_turns = jax.random.permutation(jax.random.fold_in(splits[10], 3), TOKENS // (TOK_DEV // N_TP))
    routes = jax.vmap(lambda own, number: deal_out(jax.random.fold_in(splits[10], 2), own, number, TOK_DEV // N_TP, EXPERTS, TOPK, CAP, 2))(routes_keys, routes_turns).reshape((TOKENS, TOPK))
    route_logits = noise(splits[11], (TOKENS, TOPK), 1.0, 4.0, ((0, 256),), jnp.float32)
    gate_weight = draw_gate_weight(jax.random.fold_in(splits[15], 71), 0)
    up_weight = draw_up_weight(jax.random.fold_in(splits[15], 71), 0)
    down_weight = noise(splits[14], (EXPERTS, FF, D), FF ** -0.5, 0.125, ((0, 64), (1, 4)))
    return {"residual": residual, "queries": queries, "keys": keys, "values": values, "documents": documents, "sink": sink, "out_weight": out_weight, "mix_gain": mix_gain, "ffn_gain": ffn_gain, "out_gain": out_gain, "routes": routes, "route_logits": route_logits, "gate_weight": gate_weight, "up_weight": up_weight, "down_weight": down_weight}


def turn_heads(block, positions, head_count):
    total = block.shape[0]
    heads = block.astype(jnp.float32).reshape(total, head_count, HD)
    half_size = HD // 2
    inverse = 10000.0 ** (-jnp.arange(half_size, dtype=jnp.float32) / half_size)
    angles = positions.astype(jnp.float32)[:, None] * inverse[None, :]
    cosine = jnp.cos(angles)[:, None, :]
    sine = jnp.sin(angles)[:, None, :]
    first_half = heads[..., :half_size]
    second_half = heads[..., half_size:]
    turned = jnp.concatenate([first_half * cosine - second_half * sine, second_half * cosine + first_half * sine], axis=-1)
    return turned.reshape(total, head_count * HD).astype(jnp.bfloat16)

def rms_scale(vector):
    return vector * lax.rsqrt(lax.optimization_barrier(jnp.mean(vector * vector, axis=-1, keepdims=True)) + 1e-06)

def windows(padded_rows, blocks):
    tiled = padded_rows.reshape((blocks + 2, W) + padded_rows.shape[1:])
    return jnp.concatenate([tiled[:-2], tiled[1:-1], tiled[2:]], axis=1)

def reference(residual, queries, keys, values, documents, sink, out_weight, mix_gain, ffn_gain, out_gain, routes, route_logits, gate_weight, up_weight, down_weight):
    total = TOKENS
    group_size = QH // KVH
    positions = jnp.arange(total, dtype=jnp.int32)
    q_turned = turn_heads(queries, positions, QH)
    k_turned = turn_heads(keys, positions, KVH)
    blocks = total // W
    query_blocks = q_turned.reshape(blocks, W, KVH, group_size, HD)
    key_pad = jnp.pad(k_turned.reshape(total, KVH, HD), ((W, W), (0, 0), (0, 0)))
    value_pad = jnp.pad(values.reshape(total, KVH, HD), ((W, W), (0, 0), (0, 0)))
    doc_pad = jnp.pad(documents, (W, W), constant_values=-1)
    key_win = windows(key_pad, blocks)
    value_win = windows(value_pad, blocks)
    doc_win = windows(doc_pad, blocks)
    doc_query = documents.reshape(blocks, W)
    block_ids = jnp.arange(blocks, dtype=jnp.int32)[:, None, None]
    query_pos = block_ids * W + jnp.arange(W, dtype=jnp.int32)[None, :, None]
    key_pos = (block_ids - 1) * W + jnp.arange(3 * W, dtype=jnp.int32)[None, None, :]
    keep_mask = (jnp.abs(query_pos - key_pos) <= W) & (key_pos >= 0) & (key_pos < total)
    keep_mask = keep_mask & (doc_query[:, :, None] == doc_win[:, None, :])
    sink_terms = jnp.exp(sink).reshape(KVH, group_size, 1, 1)

    def one_block(operands):
        query_one, key_one, value_one, mask_one = operands
        scores = jnp.einsum('qhgd,khd->hgqk', query_one.astype(jnp.float32), key_one.astype(jnp.float32)) * HD ** (-0.5)
        exponent = jnp.where(mask_one[None, None], jnp.exp(scores), 0.0)
        denominator = lax.optimization_barrier(jnp.sum(exponent, axis=-1, keepdims=True)) + sink_terms
        probs = (exponent / denominator).astype(jnp.bfloat16)
        attended_one = jnp.einsum('hgqk,khd->qhgd', probs.astype(jnp.float32), value_one.astype(jnp.float32))
        return attended_one.astype(jnp.bfloat16).reshape(W, QH * HD)
    attended = lax.map(one_block, (query_blocks, key_win, value_win, keep_mask)).reshape(total, QH * HD)
    projected = jnp.dot(attended, out_weight, preferred_element_type=jnp.float32)
    after_mix = residual.astype(jnp.float32) + rms_scale(projected) * mix_gain
    normed = (rms_scale(after_mix) * ffn_gain).astype(jnp.bfloat16)
    row_block = 128
    assigned = total * TOPK
    flat_routes = routes.reshape(assigned).astype(jnp.int32)
    order = jnp.argsort(flat_routes, stable=True).astype(jnp.int32)
    sorted_experts = flat_routes[order]
    sorted_tokens = (order // TOPK).astype(jnp.int32)
    counts = lax.optimization_barrier(jnp.sum((flat_routes[:, None] == jnp.arange(EXPERTS, dtype=jnp.int32)[None, :]).astype(jnp.int32), axis=0))
    padded_counts = (counts + row_block - 1) // row_block * row_block
    starts = jnp.cumsum(counts) - counts
    padded_ends = jnp.cumsum(padded_counts)
    padded_starts = padded_ends - padded_counts
    slot_rows = (padded_starts[sorted_experts] + jnp.arange(assigned, dtype=jnp.int32) - starts[sorted_experts]).astype(jnp.int32)
    block_count = -(-(assigned + EXPERTS * (row_block - 1)) // row_block)
    padded_total = block_count * row_block
    row_token = jnp.full((padded_total,), total, dtype=jnp.int32).at[slot_rows].set(sorted_tokens)
    with_zero = jnp.concatenate([normed, jnp.zeros((1, D), jnp.bfloat16)], axis=0)
    expert_rows = with_zero[row_token].reshape(block_count, row_block, D)
    block_expert = jnp.minimum(jnp.searchsorted(padded_ends, jnp.arange(block_count, dtype=jnp.int32) * row_block, side='right'), EXPERTS - 1).astype(jnp.int32)
    quarter = FF // N_TP

    def expert_block(operands):
        rows_in, expert_id = operands
        gate_pre = jnp.dot(rows_in, gate_weight[expert_id], preferred_element_type=jnp.float32)
        up_pre = jnp.dot(rows_in, up_weight[expert_id], preferred_element_type=jnp.float32)
        gated = jnp.minimum(gate_pre, 7.0)
        upper = jnp.clip(up_pre, -7.0, 7.0)
        hidden = ((upper + 1.0) * gated * jax.nn.sigmoid(1.702 * gated)).astype(jnp.bfloat16)
        down_one = down_weight[expert_id]
        summed = jnp.zeros((rows_in.shape[0], D), jnp.float32)
        for source in range(N_TP):
            partial_out = jnp.dot(hidden[:, source * quarter:(source + 1) * quarter], down_one[source * quarter:(source + 1) * quarter], preferred_element_type=jnp.float32)
            summed = summed + lax.optimization_barrier(partial_out.astype(jnp.bfloat16)).astype(jnp.float32)
        return summed.astype(jnp.bfloat16)
    expert_out = lax.map(expert_block, (expert_rows, block_expert)).reshape(padded_total, D)
    row_of = jnp.zeros((assigned,), jnp.int32).at[order].set(slot_rows).reshape(total, TOPK)
    exp_logits = jnp.exp(route_logits)
    route_weights = exp_logits / lax.optimization_barrier(jnp.sum(exp_logits, axis=-1, keepdims=True))
    expert_mix = jnp.zeros((total, D), jnp.float32)
    for choice_index in range(TOPK):
        expert_mix = expert_mix + route_weights[:, choice_index:choice_index + 1] * expert_out[row_of[:, choice_index]].astype(jnp.float32)
    return (after_mix + rms_scale(expert_mix) * out_gain).astype(jnp.bfloat16)
```

```python
import functools

import jax
import jax.numpy as jnp
from jax import lax
from jax.experimental import pallas as pl
from jax.experimental.pallas import tpu as pltpu
from jax.sharding import PartitionSpec as P

HD = 64
TOPK = 4
W = 128
D = 2048
CAP = 8
NZ, NX, NT = 8, 4, 4
NCOL = NZ * NX
MESH = pl.DeviceIdType.MESH


ORD_Z = (1, 7, 2, 6, 3, 5, 4, 0)
ORD_X = (1, 3, 2, 0)
OFFSETS = tuple((dz, dx) for dx in ORD_X for dz in ORD_Z)
SELF = OFFSETS.index((0, 0))
RANK_Z = tuple(ORD_Z.index(d) for d in range(NZ))
RANK_X = tuple(ORD_X.index(d) for d in range(NX))
GROUP = 4
GROUPS = NCOL // GROUP


def place():
    s = lax.axis_index("sp")
    t = lax.axis_index("tp")
    core = lax.rem(s, 2)
    column = lax.div(s, 2)
    return s, t, core, lax.div(column, NX), lax.rem(column, NX)


def shifted(z, x, core, dz, dx):
    return (lax.rem(z + dz, NZ) * NX + lax.rem(x + dx, NX)) * 2 + core


def greet(partners):
    barrier = pltpu.get_barrier_semaphore()
    for partner in partners:
        pl.semaphore_signal(barrier, inc=1, device_id=partner, device_id_type=MESH)
    pl.semaphore_wait(barrier, len(partners))


def partners_of(s, t, core, z, x):
    found = [(s, t + 1 - 2 * lax.rem(t, 2))]
    for index, (dz, dx) in enumerate(OFFSETS):
        column = shifted(z, x, core, dz, dx)
        found.append((column, 3 - t))
        if index != SELF:
            found.append((column, t))
    return found


def dispatch_kernel(out_ref, in_ref, send_sem, recv_sem, own_sem, far_send_sem):
    s, t, core, z, x = place()
    pair = (s, t + 1 - 2 * lax.rem(t, 2))
    greet(partners_of(s, t, core, z, x))
    own = pltpu.make_async_copy(out_ref.at[0, SELF], in_ref.at[0, SELF], own_sem)
    own.start()
    sends = []
    for index, (dz, dx) in enumerate(OFFSETS):
        column = shifted(z, x, core, dz, dx)
        for kind in range(2):
            if kind == 0 and index == SELF:
                continue
            copy = pltpu.make_async_remote_copy(
                src_ref=out_ref.at[kind, index],
                dst_ref=in_ref.at[kind, index],
                send_sem=send_sem.at[kind, index],
                recv_sem=recv_sem.at[kind, index],
                device_id=(column, t if kind == 0 else 3 - t),
                device_id_type=MESH,
            )
            copy.start()
            sends.append(copy)
    arrived = {}
    for copy, key in zip(sends, [(k, i) for i in range(NCOL) for k in range(2) if (k, i) != (0, SELF)]):
        arrived[key] = copy
    forwards = []
    for group in range(GROUPS):
        for kind in range(2):
            for index in range(group * GROUP, (group + 1) * GROUP):
                if (kind, index) == (0, SELF):
                    own.wait()
                else:
                    arrived[kind, index].wait_recv()
            block = pl.ds(group * GROUP, GROUP)
            copy = pltpu.make_async_remote_copy(
                src_ref=in_ref.at[kind, block],
                dst_ref=in_ref.at[2 + kind, block],
                send_sem=far_send_sem.at[0, kind, group],
                recv_sem=far_send_sem.at[1, kind, group],
                device_id=pair,
                device_id_type=MESH,
            )
            copy.start()
            forwards.append(copy)
    for copy in sends:
        copy.wait_send()
    for copy in forwards:
        copy.wait()


def dispatch(outgoing):
    return pl.pallas_call(
        dispatch_kernel,
        out_shape=jax.ShapeDtypeStruct((4, NCOL, CAP, D), jnp.bfloat16),
        in_specs=[pl.BlockSpec(memory_space=pltpu.VMEM)],
        out_specs=pl.BlockSpec(memory_space=pl.ANY),
        scratch_shapes=[
            pltpu.SemaphoreType.DMA((2, NCOL)),
            pltpu.SemaphoreType.DMA((2, NCOL)),
            pltpu.SemaphoreType.DMA,
            pltpu.SemaphoreType.DMA((2, 2, GROUPS)),
        ],
        compiler_params=pltpu.CompilerParams(
            collective_id=0, has_side_effects=True, vmem_limit_bytes=16 << 20
        ),
        cost_estimate=pl.CostEstimate(flops=0, bytes_accessed=150_000_000, transcendentals=0),
    )(outgoing)


def combine_kernel(terms_ref, ret_ref, mine, theirs, total, load_sem, pair_sem, send_sem, recv_sem):
    s, t, core, z, x = place()
    pair = (s, t + 1 - 2 * lax.rem(t, 2))
    greet(partners_of(s, t, core, z, x))
    pairs, loads = {}, {}
    for group in range(GROUPS):
        block = pl.ds(group * GROUP, GROUP)
        for kind in range(2):
            copy = pltpu.make_async_remote_copy(
                src_ref=terms_ref.at[2 + kind, block],
                dst_ref=theirs.at[kind, block],
                send_sem=pair_sem.at[0, kind, group],
                recv_sem=pair_sem.at[1, kind, group],
                device_id=pair,
                device_id_type=MESH,
            )
            copy.start()
            pairs[kind, group] = copy
            load = pltpu.make_async_copy(
                terms_ref.at[kind, block], mine.at[kind, block], load_sem.at[kind, group]
            )
            load.start()
            loads[kind, group] = load
    sends = []
    own = []

    def send(kind, group):
        for index in range(group * GROUP, (group + 1) * GROUP):
            dz, dx = OFFSETS[index]
            if (kind, index) == (0, SELF):
                copy = pltpu.make_async_copy(
                    total.at[kind, index], ret_ref.at[kind, index], send_sem.at[kind, index]
                )
                own.append(copy)
            else:
                column = shifted(z, x, core, NZ - dz, NX - dx)
                copy = pltpu.make_async_remote_copy(
                    src_ref=total.at[kind, index],
                    dst_ref=ret_ref.at[kind, index],
                    send_sem=send_sem.at[kind, index],
                    recv_sem=recv_sem.at[kind, index],
                    device_id=(column, t if kind == 0 else 3 - t),
                    device_id_type=MESH,
                )
                sends.append(copy)
            copy.start()

    steps = [(kind, group) for group in range(GROUPS) for kind in range(2)]
    for number, (kind, group) in enumerate(steps):
        block = pl.ds(group * GROUP, GROUP)
        loads[kind, group].wait()
        pairs[kind, group].wait_recv()
        total[kind, block] = (
            mine[kind, block].astype(jnp.float32) + theirs[kind, block].astype(jnp.float32)
        ).astype(jnp.bfloat16)
        if number:
            send(*steps[number - 1])
    send(*steps[-1])
    for copy in pairs.values():
        copy.wait_send()
    for copy in own:
        copy.wait()
    for copy in sends:
        copy.wait()


def combine(terms):
    half = (2, NCOL, CAP, D)
    return pl.pallas_call(
        combine_kernel,
        out_shape=jax.ShapeDtypeStruct(half, jnp.bfloat16),
        in_specs=[pl.BlockSpec(memory_space=pl.ANY)],
        out_specs=pl.BlockSpec(memory_space=pl.ANY),
        scratch_shapes=[
            pltpu.VMEM(half, jnp.bfloat16),
            pltpu.VMEM(half, jnp.bfloat16),
            pltpu.VMEM(half, jnp.bfloat16),
            pltpu.SemaphoreType.DMA((2, GROUPS)),
            pltpu.SemaphoreType.DMA((2, 2, GROUPS)),
            pltpu.SemaphoreType.DMA((2, NCOL)),
            pltpu.SemaphoreType.DMA((2, NCOL)),
        ],
        compiler_params=pltpu.CompilerParams(
            collective_id=1, has_side_effects=True, vmem_limit_bytes=16 << 20
        ),
        cost_estimate=pl.CostEstimate(flops=0, bytes_accessed=150_000_000, transcendentals=0),
    )(terms)


def weight_moves(sp_count):
    first, second = [], []
    for s in range(sp_count):
        for t in range(NT):
            core, side = s % 2, t // 2
            sibling = (s ^ 1) * NT + t
            second.append((s * NT + t, sibling))
            first.append((s * NT + t, sibling if core == side else s * NT + 3 - t))
    return first, second


def extended(block, sides, width):
    for axis, dim in sides:
        count = lax.axis_size(axis)
        forward = [(i, i + 1) for i in range(count - 1)]
        backward = [(target, source) for source, target in forward]
        low = lax.ppermute(
            lax.slice_in_dim(block, block.shape[dim] - width, None, axis=dim), axis, forward
        )
        high = lax.ppermute(lax.slice_in_dim(block, 0, width, axis=dim), axis, backward)
        block = jnp.concatenate([low, block, high], axis=dim)
    return block


def turn_heads(block, positions, head_count):
    total = block.shape[0]
    heads = block.astype(jnp.float32).reshape(total, head_count, HD)
    half_size = HD // 2
    inverse = 10000.0 ** (-jnp.arange(half_size, dtype=jnp.float32) / half_size)
    angles = positions.astype(jnp.float32)[:, None] * inverse[None, :]
    cosine = jnp.cos(angles)[:, None, :]
    sine = jnp.sin(angles)[:, None, :]
    first_half = heads[..., :half_size]
    second_half = heads[..., half_size:]
    turned = jnp.concatenate(
        [first_half * cosine - second_half * sine, second_half * cosine + first_half * sine],
        axis=-1,
    )
    return turned.reshape(total, head_count * HD).astype(jnp.bfloat16)


def rms_scale(vector):
    return vector * lax.rsqrt(jnp.mean(vector * vector, axis=-1, keepdims=True) + 1e-06)


def windows(padded_rows, blocks):
    tiled = padded_rows.reshape((blocks + 2, W) + padded_rows.shape[1:])
    return jnp.concatenate([tiled[:-2], tiled[1:-1], tiled[2:]], axis=1)


def slots(route_rows, expert_count):
    flat_routes = route_rows.reshape(route_rows.shape[0] * TOPK)
    onehot_hits = (
        flat_routes[:, None] == jnp.arange(expert_count, dtype=jnp.int32)[None, :]
    ).astype(jnp.int32)
    slot_number = jnp.sum(jnp.cumsum(onehot_hits, axis=0) * onehot_hits, axis=1) - 1
    s, t, core, z, x = place()
    column = flat_routes // 2
    dz = (column // NX - z + NZ) % NZ
    dx = (column % NX - x + NX) % NX
    rank_z, rank_x = jnp.zeros_like(dz), jnp.zeros_like(dx)
    for d in range(NZ):
        rank_z = jnp.where(dz == d, RANK_Z[d], rank_z)
    for d in range(NX):
        rank_x = jnp.where(dx == d, RANK_X[d], rank_x)
    kind = jnp.where(flat_routes % 2 == t // 2, 0, 1)
    position = ((kind * NX + rank_x) * NZ + rank_z) * CAP + slot_number
    return position.reshape(route_rows.shape)


def body(
    residual,
    queries,
    keys,
    values,
    documents,
    sink,
    out_weight,
    mix_gain,
    ffn_gain,
    out_gain,
    routes,
    route_logits,
    gate_weight,
    up_weight,
    down_weight,
):
    tok_rows = queries.shape[0]
    head_count = queries.shape[1] // HD
    kv_count = keys.shape[1] // HD
    group_size = head_count // kv_count
    sp_count = lax.axis_size("sp")
    tp_count = lax.axis_size("tp")
    first, second = weight_moves(sp_count)
    halves = []
    for weight in (gate_weight[0], up_weight[0], down_weight[0]):
        one = lax.ppermute(weight, ("sp", "tp"), first)
        two = lax.ppermute(one, ("sp", "tp"), second)
        halves.append((one, two))
    offset = lax.axis_index("sp") * tok_rows
    positions = offset + jnp.arange(tok_rows, dtype=jnp.int32)
    q_turned = turn_heads(queries, positions, head_count)
    k_turned = turn_heads(keys, positions, kv_count)
    paired = jnp.concatenate([k_turned, values], axis=1)
    wide_pairs, wide_docs = (
        extended(paired, (("sp", 0),), W),
        extended(documents, (("sp", 0),), W),
    )
    blocks = tok_rows // W
    query_blocks = q_turned.reshape(blocks, W, kv_count, group_size, HD)
    pair_win = windows(wide_pairs, blocks)
    key_win = pair_win[..., : kv_count * HD].reshape(blocks, 3 * W, kv_count, HD)
    value_win = pair_win[..., kv_count * HD :].reshape(blocks, 3 * W, kv_count, HD)
    doc_win = windows(wide_docs, blocks)
    doc_query = documents.reshape(blocks, W)
    block_ids = jnp.arange(blocks, dtype=jnp.int32)[:, None, None]
    query_pos = offset + block_ids * W + jnp.arange(W, dtype=jnp.int32)[None, :, None]
    key_pos = offset + (block_ids - 1) * W + jnp.arange(3 * W, dtype=jnp.int32)[None, None, :]
    keep_mask = (
        (jnp.abs(query_pos - key_pos) <= W) & (key_pos >= 0) & (key_pos < tok_rows * sp_count)
    )
    keep_mask = keep_mask & (doc_query[:, :, None] == doc_win[:, None, :])
    scores = jnp.einsum(
        "nqhgd,nkhd->nhgqk", query_blocks, key_win, preferred_element_type=jnp.float32
    ) * HD ** (-0.5)
    exponent = jnp.where(keep_mask[:, None, None], jnp.exp(scores), 0.0)
    denominator = jnp.sum(exponent, axis=-1, keepdims=True) + jnp.exp(sink).reshape(
        1, kv_count, group_size, 1, 1
    )
    probs = (exponent / denominator).astype(jnp.bfloat16)
    attended = jnp.einsum("nhgqk,nkhd->nqhgd", probs, value_win, preferred_element_type=jnp.float32)
    attended = attended.astype(jnp.bfloat16).reshape(tok_rows, head_count * HD)
    own_rows = tok_rows // tp_count
    all_heads = lax.all_to_all(attended, "tp", split_axis=0, concat_axis=1, tiled=True)
    projected = jnp.dot(all_heads, out_weight, preferred_element_type=jnp.float32)
    after_mix = residual.astype(jnp.float32) + rms_scale(projected) * mix_gain
    normed = (rms_scale(after_mix) * ffn_gain).astype(jnp.bfloat16)
    expert_count = gate_weight.shape[0] * sp_count
    position = slots(routes, expert_count)
    hits = position[:, :, None] == jnp.arange(expert_count * CAP, dtype=jnp.int32)
    picks = jnp.any(hits, axis=1).astype(jnp.bfloat16)
    outgoing = lax.dot_general(
        picks, normed, (((0,), (0,)), ((), ())), preferred_element_type=jnp.float32
    ).astype(jnp.bfloat16)
    rows_in = dispatch(outgoing.reshape(2, NCOL, CAP, D)).reshape(4 * NCOL * CAP, D)
    terms = 0.0
    for which in range(2):
        gate_half, up_half, down_half = (half[which] for half in halves)
        gate_pre = jnp.dot(rows_in, gate_half, preferred_element_type=jnp.float32)
        up_pre = jnp.dot(rows_in, up_half, preferred_element_type=jnp.float32)
        gated = jnp.minimum(gate_pre, 7.0)
        upper = jnp.clip(up_pre, -7.0, 7.0)
        hidden = ((upper + 1.0) * gated * jax.nn.sigmoid(1.702 * gated)).astype(jnp.bfloat16)
        terms = terms + jnp.dot(hidden, down_half, preferred_element_type=jnp.float32)
    returned = combine(terms.astype(jnp.bfloat16).reshape(4, NCOL, CAP, D))
    returned = returned.reshape(expert_count * CAP, D)
    exp_logits = jnp.exp(route_logits)
    route_weights = exp_logits / jnp.sum(exp_logits, axis=-1, keepdims=True)
    spread = jnp.sum(jnp.where(hits, route_weights[:, :, None], 0.0), axis=1)
    coarse = lax.reduce_precision(spread, 8, 7)
    expert_mix = jnp.dot(
        coarse.astype(jnp.bfloat16), returned, preferred_element_type=jnp.float32
    ) + jnp.dot(
        (spread - coarse).astype(jnp.bfloat16), returned, preferred_element_type=jnp.float32
    )
    return (after_mix + rms_scale(expert_mix) * out_gain).astype(jnp.bfloat16)


def solution(mesh):
    in_specs = (
        P(("sp", "tp"), None),
        P("sp", "tp"),
        P("sp", "tp"),
        P("sp", "tp"),
        P("sp"),
        P("tp"),
        P(),
        P(),
        P(),
        P(),
        P(("sp", "tp"), None),
        P(("sp", "tp"), None),
        P("sp", None, "tp"),
        P("sp", None, "tp"),
        P("sp", "tp", None),
    )
    out_specs = P(("sp", "tp"), None)
    return jax.shard_map(body, mesh=mesh, in_specs=in_specs, out_specs=out_specs, check_vma=False)
```

```python
import jax
import jax.numpy as jnp
from jax import lax
from jax.experimental import pallas as pl
from jax.experimental.pallas import tpu as pltpu
from jax.sharding import PartitionSpec as P

HD = 64
TOPK = 4
W = 128
D = 2048
CAP = 8
NZ, NX, NT = 8, 4, 4
NCOL = NZ * NX
MESH = pl.DeviceIdType.MESH


NEAR_Z = (1, 7, 2, 6, 3, 5)
OFFSETS = (
    tuple((0, dx) for dx in (1, 3, 2, 0))
    + tuple((dz, dx) for dx in (1, 3) for dz in NEAR_Z)
    + tuple((4, dx) for dx in (1, 3, 2, 0))
    + tuple((dz, dx) for dx in (2, 0) for dz in NEAR_Z)
)
SELF = OFFSETS.index((0, 0))
GROUP = 4
GROUPS = NCOL // GROUP
BACK = (4, 1, 2, 3, 5, 6, 7, 0)
HALF = 512
TILE = 256


def place():
    s = lax.axis_index("sp")
    t = lax.axis_index("tp")
    core = lax.rem(s, 2)
    column = lax.div(s, 2)
    return s, t, core, lax.div(column, NX), lax.rem(column, NX)


def shifted(z, x, core, dz, dx):
    return (lax.rem(z + dz, NZ) * NX + lax.rem(x + dx, NX)) * 2 + core


def greet(partners):
    barrier = pltpu.get_barrier_semaphore()
    for partner in partners:
        pl.semaphore_signal(barrier, inc=1, device_id=partner, device_id_type=MESH)
    pl.semaphore_wait(barrier, len(partners))


def partners_of(s, t, core, z, x):
    found = [(s, t + 1 - 2 * lax.rem(t, 2))]
    for index, (dz, dx) in enumerate(OFFSETS):
        column = shifted(z, x, core, dz, dx)
        found.append((column, 3 - t))
        if index != SELF:
            found.append((column, t))
    return found


def dispatch_kernel(out_ref, in_ref, send_sem, recv_sem, own_sem, far_send_sem):
    s, t, core, z, x = place()
    pair = (s, t + 1 - 2 * lax.rem(t, 2))
    greet(partners_of(s, t, core, z, x))
    own = pltpu.make_async_copy(out_ref.at[0, SELF], in_ref.at[0, SELF], own_sem)
    own.start()
    sends = []
    for index, (dz, dx) in enumerate(OFFSETS):
        column = shifted(z, x, core, dz, dx)
        for kind in range(2):
            if kind == 0 and index == SELF:
                continue
            copy = pltpu.make_async_remote_copy(
                src_ref=out_ref.at[kind, index],
                dst_ref=in_ref.at[kind, index],
                send_sem=send_sem.at[kind, index],
                recv_sem=recv_sem.at[kind, index],
                device_id=(column, t if kind == 0 else 3 - t),
                device_id_type=MESH,
            )
            copy.start()
            sends.append(copy)
    arrived = {}
    for copy, key in zip(sends, [(k, i) for i in range(NCOL) for k in range(2) if (k, i) != (0, SELF)]):
        arrived[key] = copy
    forwards = []
    for group in range(GROUPS):
        for kind in range(2):
            for index in range(group * GROUP, (group + 1) * GROUP):
                if (kind, index) == (0, SELF):
                    own.wait()
                else:
                    arrived[kind, index].wait_recv()
            block = pl.ds(group * GROUP, GROUP)
            copy = pltpu.make_async_remote_copy(
                src_ref=in_ref.at[kind, block],
                dst_ref=in_ref.at[2 + kind, block],
                send_sem=far_send_sem.at[0, kind, group],
                recv_sem=far_send_sem.at[1, kind, group],
                device_id=pair,
                device_id_type=MESH,
            )
            copy.start()
            forwards.append(copy)
    for copy in sends:
        copy.wait_send()
    for copy in forwards:
        copy.wait()


def dispatch(outgoing):
    return pl.pallas_call(
        dispatch_kernel,
        out_shape=jax.ShapeDtypeStruct((4, NCOL, CAP, D), jnp.bfloat16),
        in_specs=[pl.BlockSpec(memory_space=pltpu.VMEM)],
        out_specs=pl.BlockSpec(memory_space=pl.ANY),
        scratch_shapes=[
            pltpu.SemaphoreType.DMA((2, NCOL)),
            pltpu.SemaphoreType.DMA((2, NCOL)),
            pltpu.SemaphoreType.DMA,
            pltpu.SemaphoreType.DMA((2, 2, GROUPS)),
        ],
        compiler_params=pltpu.CompilerParams(
            collective_id=0, has_side_effects=True, vmem_limit_bytes=16 << 20
        ),
        cost_estimate=pl.CostEstimate(flops=0, bytes_accessed=150_000_000, transcendentals=0),
    )(outgoing)


def expert_kernel(
    rows_ref,
    gate_one,
    gate_two,
    up_one,
    up_two,
    down_one,
    down_two,
    ret_ref,
    block_rows,
    hidden,
    mine,
    away,
    theirs,
    total,
    pair_sem,
    send_sem,
    recv_sem,
):
    s, t, core, z, x = place()
    pair = (s, t + 1 - 2 * lax.rem(t, 2))
    greet(partners_of(s, t, core, z, x))
    count = 4 * GROUP * CAP
    pairs = {}
    sends = []
    own = []

    def activate(gate, up, target, column):
        columns = pl.ds(pl.multiple_of(column * TILE, TILE), TILE)
        gate_pre = jnp.dot(block_rows[...], gate[:, columns], preferred_element_type=jnp.float32)
        up_pre = jnp.dot(block_rows[...], up[:, columns], preferred_element_type=jnp.float32)
        gated = jnp.minimum(gate_pre, 7.0)
        upper = jnp.clip(up_pre, -7.0, 7.0)
        value = (upper + 1.0) * gated * jax.nn.sigmoid(1.702 * gated)
        columns = pl.ds(pl.multiple_of(target * HALF + column * TILE, TILE), TILE)
        hidden[:, columns] = value.astype(jnp.bfloat16)

    def compute(group):
        block = pl.ds(group * GROUP, GROUP)
        block_rows[...] = (
            rows_ref[:, block].astype(jnp.float32).reshape(count, D).astype(jnp.bfloat16)
        )

        @pl.loop(0, HALF // TILE)
        def _(column):
            activate(gate_one, up_one, 0, column)
            activate(gate_two, up_two, 1, column)

        @pl.loop(0, D // TILE)
        def _(column):
            columns = pl.ds(pl.multiple_of(column * TILE, TILE), TILE)
            term = jnp.dot(
                hidden[:, :HALF], down_one[:, columns], preferred_element_type=jnp.float32
            ) + jnp.dot(hidden[:, HALF:], down_two[:, columns], preferred_element_type=jnp.float32)
            term = term.reshape(4, GROUP, CAP, TILE).astype(jnp.bfloat16)
            mine[:, block, :, columns] = term[:2]
            away[:, block, :, columns] = term[2:]

    def swap(group):
        block = pl.ds(group * GROUP, GROUP)
        for kind in (1, 0):
            copy = pltpu.make_async_remote_copy(
                src_ref=away.at[kind, block],
                dst_ref=theirs.at[kind, block],
                send_sem=pair_sem.at[0, kind, group],
                recv_sem=pair_sem.at[1, kind, group],
                device_id=pair,
                device_id_type=MESH,
            )
            copy.start()
            pairs[kind, group] = copy

    def add(group):
        block = pl.ds(group * GROUP, GROUP)
        for kind in (1, 0):
            pairs[kind, group].wait_recv()
            total[kind, block] = (
                mine[kind, block].astype(jnp.float32) + theirs[kind, block].astype(jnp.float32)
            ).astype(jnp.bfloat16)

    def home(group):
        for kind in (1, 0):
            for index in range(group * GROUP, (group + 1) * GROUP):
                dz, dx = OFFSETS[index]
                if (kind, index) == (0, SELF):
                    copy = pltpu.make_async_copy(
                        total.at[kind, index], ret_ref.at[kind, index], send_sem.at[kind, index]
                    )
                    own.append(copy)
                else:
                    column = shifted(z, x, core, NZ - dz, NX - dx)
                    copy = pltpu.make_async_remote_copy(
                        src_ref=total.at[kind, index],
                        dst_ref=ret_ref.at[kind, index],
                        send_sem=send_sem.at[kind, index],
                        recv_sem=recv_sem.at[kind, index],
                        device_id=(column, t if kind == 0 else 3 - t),
                        device_id_type=MESH,
                    )
                    sends.append(copy)
                copy.start()

    behind = 2
    for step in range(GROUPS + behind):
        if step < GROUPS:
            compute(BACK[step])
        if step >= behind:
            add(BACK[step - behind])
        if step < GROUPS:
            swap(BACK[step])
        if step >= behind:
            home(BACK[step - behind])
    for copy in pairs.values():
        copy.wait_send()
    for copy in own:
        copy.wait()
    for copy in sends:
        copy.wait()


def expert_outputs(rows_in, halves):
    half = (2, NCOL, CAP, D)
    flat = [one for pair in halves for one in pair]
    vmem = pl.BlockSpec(memory_space=pltpu.VMEM)
    return pl.pallas_call(
        expert_kernel,
        out_shape=jax.ShapeDtypeStruct(half, jnp.bfloat16),
        in_specs=[vmem] * 7,
        out_specs=pl.BlockSpec(memory_space=pl.ANY),
        scratch_shapes=[
            pltpu.VMEM((4 * GROUP * CAP, D), jnp.bfloat16),
            pltpu.VMEM((4 * GROUP * CAP, 2 * HALF), jnp.bfloat16),
            pltpu.VMEM(half, jnp.bfloat16),
            pltpu.VMEM(half, jnp.bfloat16),
            pltpu.VMEM(half, jnp.bfloat16),
            pltpu.VMEM(half, jnp.bfloat16),
            pltpu.SemaphoreType.DMA((2, 2, GROUPS)),
            pltpu.SemaphoreType.DMA((2, NCOL)),
            pltpu.SemaphoreType.DMA((2, NCOL)),
        ],
        compiler_params=pltpu.CompilerParams(
            collective_id=1, has_side_effects=True, vmem_limit_bytes=40 << 20
        ),
        cost_estimate=pl.CostEstimate(
            flops=13_000_000_000, bytes_accessed=150_000_000, transcendentals=0
        ),
    )(rows_in, *flat)


def weight_moves(sp_count):
    first, second = [], []
    for s in range(sp_count):
        for t in range(NT):
            core, side = s % 2, t // 2
            sibling = (s ^ 1) * NT + t
            second.append((s * NT + t, sibling))
            first.append((s * NT + t, sibling if core == side else s * NT + 3 - t))
    return first, second


def extended(block, sides, width):
    for axis, dim in sides:
        count = lax.axis_size(axis)
        forward = [(i, i + 1) for i in range(count - 1)]
        backward = [(target, source) for source, target in forward]
        low = lax.ppermute(
            lax.slice_in_dim(block, block.shape[dim] - width, None, axis=dim), axis, forward
        )
        high = lax.ppermute(lax.slice_in_dim(block, 0, width, axis=dim), axis, backward)
        block = jnp.concatenate([low, block, high], axis=dim)
    return block


def turn_heads(block, positions, head_count):
    total = block.shape[0]
    heads = block.astype(jnp.float32).reshape(total, head_count, HD)
    half_size = HD // 2
    inverse = 10000.0 ** (-jnp.arange(half_size, dtype=jnp.float32) / half_size)
    angles = positions.astype(jnp.float32)[:, None] * inverse[None, :]
    cosine = jnp.cos(angles)[:, None, :]
    sine = jnp.sin(angles)[:, None, :]
    first_half = heads[..., :half_size]
    second_half = heads[..., half_size:]
    turned = jnp.concatenate(
        [first_half * cosine - second_half * sine, second_half * cosine + first_half * sine],
        axis=-1,
    )
    return turned.reshape(total, head_count * HD).astype(jnp.bfloat16)


def rms_scale(vector):
    return vector * lax.rsqrt(jnp.mean(vector * vector, axis=-1, keepdims=True) + 1e-06)


def windows(padded_rows, blocks):
    tiled = padded_rows.reshape((blocks + 2, W) + padded_rows.shape[1:])
    return jnp.concatenate([tiled[:-2], tiled[1:-1], tiled[2:]], axis=1)


def slots(route_rows, expert_count):
    flat_routes = route_rows.reshape(route_rows.shape[0] * TOPK)
    onehot_hits = (
        flat_routes[:, None] == jnp.arange(expert_count, dtype=jnp.int32)[None, :]
    ).astype(jnp.int32)
    slot_number = jnp.sum(jnp.cumsum(onehot_hits, axis=0) * onehot_hits, axis=1) - 1
    _, t, _, z, x = place()
    column = flat_routes // 2
    dz = (column // NX - z + NZ) % NZ
    dx = (column % NX - x + NX) % NX
    rank = jnp.zeros_like(dz)
    for index, (far_z, far_x) in enumerate(OFFSETS):
        rank = jnp.where((dz == far_z) & (dx == far_x), index, rank)
    kind = jnp.where(flat_routes % 2 == t // 2, 0, 1)
    position = (kind * NCOL + rank) * CAP + slot_number
    return position.reshape(route_rows.shape)


def body(
    residual,
    queries,
    keys,
    values,
    documents,
    sink,
    out_weight,
    mix_gain,
    ffn_gain,
    out_gain,
    routes,
    route_logits,
    gate_weight,
    up_weight,
    down_weight,
):
    tok_rows = queries.shape[0]
    head_count = queries.shape[1] // HD
    kv_count = keys.shape[1] // HD
    group_size = head_count // kv_count
    sp_count = lax.axis_size("sp")
    first, second = weight_moves(sp_count)
    gate_one = lax.ppermute(gate_weight[0], ("sp", "tp"), first)
    offset = lax.axis_index("sp") * tok_rows
    positions = offset + jnp.arange(tok_rows, dtype=jnp.int32)
    q_turned = turn_heads(queries, positions, head_count)
    k_turned = turn_heads(keys, positions, kv_count)
    paired = jnp.concatenate([k_turned, values], axis=1)
    wide_pairs, wide_docs = (
        extended(paired, (("sp", 0),), W),
        extended(documents, (("sp", 0),), W),
    )
    blocks = tok_rows // W
    query_blocks = q_turned.reshape(blocks, W, kv_count, group_size, HD)
    pair_win = windows(wide_pairs, blocks)
    key_win = pair_win[..., : kv_count * HD].reshape(blocks, 3 * W, kv_count, HD)
    value_win = pair_win[..., kv_count * HD :].reshape(blocks, 3 * W, kv_count, HD)
    doc_win = windows(wide_docs, blocks)
    doc_query = documents.reshape(blocks, W)
    block_ids = jnp.arange(blocks, dtype=jnp.int32)[:, None, None]
    query_pos = offset + block_ids * W + jnp.arange(W, dtype=jnp.int32)[None, :, None]
    key_pos = offset + (block_ids - 1) * W + jnp.arange(3 * W, dtype=jnp.int32)[None, None, :]
    keep_mask = (
        (jnp.abs(query_pos - key_pos) <= W) & (key_pos >= 0) & (key_pos < tok_rows * sp_count)
    )
    keep_mask = keep_mask & (doc_query[:, :, None] == doc_win[:, None, :])
    scores = jnp.einsum(
        "nqhgd,nkhd->nhgqk", query_blocks, key_win, preferred_element_type=jnp.float32
    ) * HD ** (-0.5)
    exponent = jnp.where(keep_mask[:, None, None], jnp.exp(scores), 0.0)
    denominator = jnp.sum(exponent, axis=-1, keepdims=True) + jnp.exp(sink).reshape(
        1, kv_count, group_size, 1, 1
    )
    probs = (exponent / denominator).astype(jnp.bfloat16)
    attended = jnp.einsum("nhgqk,nkhd->nqhgd", probs, value_win, preferred_element_type=jnp.float32)
    attended = attended.astype(jnp.bfloat16).reshape(tok_rows, head_count * HD)
    all_heads = lax.all_to_all(attended, "tp", split_axis=0, concat_axis=1, tiled=True)
    all_heads, up_weight, down_weight = lax.optimization_barrier(
        (all_heads, up_weight, down_weight)
    )
    up_one = lax.ppermute(up_weight[0], ("sp", "tp"), first)
    down_one = lax.ppermute(down_weight[0], ("sp", "tp"), first)
    gate_two = lax.ppermute(gate_one, ("sp", "tp"), second)
    projected = jnp.dot(all_heads, out_weight, preferred_element_type=jnp.float32)
    after_mix = residual.astype(jnp.float32) + rms_scale(projected) * mix_gain
    normed = (rms_scale(after_mix) * ffn_gain).astype(jnp.bfloat16)
    expert_count = gate_weight.shape[0] * sp_count
    position = slots(routes, expert_count)
    hits = position[:, :, None] == jnp.arange(expert_count * CAP, dtype=jnp.int32)
    picks = jnp.any(hits, axis=1).astype(jnp.bfloat16)
    outgoing = lax.dot_general(
        picks, normed, (((0,), (0,)), ((), ())), preferred_element_type=jnp.float32
    ).astype(jnp.bfloat16)
    rows_in = dispatch(outgoing.reshape(2, NCOL, CAP, D))
    up_two = lax.ppermute(up_one, ("sp", "tp"), second)
    down_two = lax.ppermute(down_one, ("sp", "tp"), second)
    halves = ((gate_one, gate_two), (up_one, up_two), (down_one, down_two))
    returned = expert_outputs(rows_in, halves)
    returned = returned.reshape(expert_count * CAP, D)
    exp_logits = jnp.exp(route_logits)
    route_weights = exp_logits / jnp.sum(exp_logits, axis=-1, keepdims=True)
    spread = jnp.sum(jnp.where(hits, route_weights[:, :, None], 0.0), axis=1)
    coarse = lax.reduce_precision(spread, 8, 7)
    expert_mix = jnp.dot(
        coarse.astype(jnp.bfloat16), returned, preferred_element_type=jnp.float32
    ) + jnp.dot(
        (spread - coarse).astype(jnp.bfloat16), returned, preferred_element_type=jnp.float32
    )
    return (after_mix + rms_scale(expert_mix) * out_gain).astype(jnp.bfloat16)


def solution(mesh):
    in_specs = (
        P(("sp", "tp"), None),
        P("sp", "tp"),
        P("sp", "tp"),
        P("sp", "tp"),
        P("sp"),
        P("tp"),
        P(),
        P(),
        P(),
        P(),
        P(("sp", "tp"), None),
        P(("sp", "tp"), None),
        P("sp", None, "tp"),
        P("sp", None, "tp"),
        P("sp", "tp", None),
    )
    out_specs = P(("sp", "tp"), None)

    return jax.shard_map(body, mesh=mesh, in_specs=in_specs, out_specs=out_specs, check_vma=False)
```

```python
import functools

import jax
import jax.numpy as jnp
from jax import lax
from jax.experimental import pallas as pl
from jax.experimental.pallas import tpu as pltpu
from jax.sharding import PartitionSpec as P

HD = 64
TOPK = 4
W = 128
D = 2048
CAP = 8
NZ, NX, NT = 8, 4, 4
NCOL = NZ * NX
MESH = pl.DeviceIdType.MESH

NEAR_Z = (1, 7, 2, 6, 3, 5)
OFFSETS = (
    tuple((0, dx) for dx in (1, 3, 2, 0))
    + tuple((dz, dx) for dx in (1, 3) for dz in NEAR_Z)
    + tuple((4, dx) for dx in (1, 3, 2, 0))
    + tuple((dz, dx) for dx in (2, 0) for dz in NEAR_Z)
)
SELF = OFFSETS.index((0, 0))
GROUP = 4
GROUPS = NCOL // GROUP
BACK = (4, 1, 2, 3, 5, 6, 7, 0)
TILE = 256
ROWS = 96
SPAN = 384
SLOTS = 2 * NCOL * CAP
NS = 2 * NCOL


def place():
    s = lax.axis_index("sp")
    t = lax.axis_index("tp")
    core = lax.rem(s, 2)
    column = lax.div(s, 2)
    return s, t, core, lax.div(column, NX), lax.rem(column, NX)


def shifted(z, x, core, dz, dx):
    return (lax.rem(z + dz, NZ) * NX + lax.rem(x + dx, NX)) * 2 + core


def greet(partners):
    barrier = pltpu.get_barrier_semaphore()
    for partner in partners:
        pl.semaphore_signal(barrier, inc=1, device_id=partner, device_id_type=MESH)
    pl.semaphore_wait(barrier, len(partners))


def mates(s, t):
    return [(s, lax.rem(t + step, NT)) for step in (1, 2, 3)]


def partners_of(s, t, core, z, x):
    found = mates(s, t)
    for index, (dz, dx) in enumerate(OFFSETS):
        if index != SELF:
            found.append((shifted(z, x, core, dz, dx), t))
    return found


def remote(source, target, send_sem, recv_sem, device):
    copy = pltpu.make_async_remote_copy(
        src_ref=source,
        dst_ref=target,
        send_sem=send_sem,
        recv_sem=recv_sem,
        device_id=device,
        device_id_type=MESH,
    )
    copy.start()
    return copy


def attention_kernel(
    cos_ref,
    sin_ref,
    aux_ref,
    q_hbm,
    k_hbm,
    v_hbm,
    wo_hbm,
    res_hbm,
    mix_hbm,
    ffn_hbm,
    routes_hbm,
    logits_hbm,
    gate_ref,
    up_ref,
    down_ref,
    after_ref,
    outgoing_ref,
    coarse_ref,
    fine_ref,
    gate_out,
    up_out,
    down_out,
    q_ref,
    kv_ref,
    wo_buf,
    res_ref,
    mix_ref,
    ffn_ref,
    routes_ref,
    logits_ref,
    kv_ext,
    doc_ext,
    attended,
    heads,
    normed,
    picks_buf,
    load_sem,
    halo_sem,
    head_sem,
    move_sem,
    swap_sem,
):
    s, t, core, z, x = place()
    above = (lax.rem(s + 1, NS), t)
    below = (lax.rem(s + NS - 1, NS), t)
    sibling = (s + 1 - 2 * core, t)
    keeper = core == lax.rem(t, 2)
    barrier = pltpu.get_barrier_semaphore()
    found = [above, below] + mates(s, t)
    for partner in found:
        pl.semaphore_signal(barrier, inc=1, device_id=partner, device_id_type=MESH)
    loads = [
        pltpu.make_async_copy(source, target, load_sem.at[number])
        for number, (source, target) in enumerate(
            (
                (k_hbm, kv_ref.at[pl.ds(0, HD)]),
                (v_hbm, kv_ref.at[pl.ds(HD, HD)]),
                (q_hbm, q_ref),
                (routes_hbm, routes_ref),
                (logits_hbm, logits_ref),
                (wo_hbm, wo_buf),
                (res_hbm, res_ref),
                (mix_hbm, mix_ref),
                (ffn_hbm, ffn_ref),
            )
        )
    ]
    for load in loads:
        load.start()
    pl.semaphore_wait(barrier, len(found))

    moves = {}

    def move(which):
        for side, step in ((0, 1), (1, 3)):
            neighbour = lax.rem(t + step, NT)
            half = jnp.where(keeper, side, lax.div(neighbour, 2))
            device = (jnp.where(keeper, sibling[0], s), jnp.where(keeper, t, neighbour))
            piece = pl.ds(pl.multiple_of(half * TILE, TILE), TILE)
            if which == 2:
                source, target = down_ref.at[piece, :], down_out.at[2 + side]
            elif which == 1:
                source, target = up_ref.at[:, piece], up_out.at[2 + side]
            else:
                source, target = gate_ref.at[:, piece], gate_out.at[2 + side]
            moves[which, side] = remote(
                source, target, move_sem.at[0, which, side], move_sem.at[1, which, side], device
            )

    move(0)
    move(1)
    for load in loads[:3]:
        load.wait()

    lane = lax.broadcasted_iota(jnp.int32, (128, 128), 1)
    low_half = (lane & 32) == 0
    left = lane < 64

    def turned(value, cosine, sine):
        swapped = jnp.where(low_half, pltpu.roll(value, 96, 1), pltpu.roll(value, 32, 1))
        return value * cosine + swapped * sine

    for block in (0, 2, 1):
        rows = pl.ds(block * W, W)
        pair = kv_ref[:, block * W : block * W + W].astype(jnp.float32).T
        key_turned = turned(pair, cos_ref[rows, :], sin_ref[rows, :])
        kv_ext[block + 1] = jnp.where(left, key_turned, pair).astype(jnp.bfloat16)
        doc_ext[block + 1] = aux_ref[block : block + 1, :]
    halos = [
        remote(kv_ext.at[1], kv_ext.at[4], halo_sem.at[0, 0], halo_sem.at[1, 0], below),
        remote(kv_ext.at[3], kv_ext.at[0], halo_sem.at[0, 1], halo_sem.at[1, 1], above),
        remote(doc_ext.at[1], doc_ext.at[4], halo_sem.at[0, 2], halo_sem.at[1, 2], below),
        remote(doc_ext.at[3], doc_ext.at[0], halo_sem.at[0, 3], halo_sem.at[1, 3], above),
    ]

    contract = (((1,), (1,)), ((), ()))
    for block in (1, 0, 2):
        if block == 0:
            for halo in halos:
                halo.wait_recv()
        rows = pl.ds(block * W, W)
        keys_low, keys_high, vals_low, vals_high, keep = [], [], [], [], []
        doc_query = jnp.broadcast_to(aux_ref[block : block + 1, :], (128, 128)).T
        for part in range(3):
            pair = kv_ext[block + part].astype(jnp.float32)
            other = pltpu.roll(pair, 64, 1)
            keys_low.append(jnp.where(left, pair, 0.0).astype(jnp.bfloat16))
            keys_high.append(jnp.where(left, 0.0, other).astype(jnp.bfloat16))
            vals_low.append(jnp.where(left, other, 0.0).astype(jnp.bfloat16))
            vals_high.append(jnp.where(left, 0.0, pair).astype(jnp.bfloat16))
            gap = (part - 1) * W + lane - lax.broadcasted_iota(jnp.int32, (128, 128), 0)
            place_of = s * SPAN + (block + part - 1) * W + lane
            doc_key = doc_ext[block + part]
            keep.append(
                (jnp.abs(gap) <= W)
                & (place_of >= 0)
                & (place_of < NS * SPAN)
                & (doc_query == doc_key)
            )
        keep = jnp.concatenate(keep, axis=1)
        keys_of = [jnp.concatenate(part, axis=0) for part in (keys_low, keys_high)]
        vals_of = [jnp.concatenate(part, axis=0) for part in (vals_low, vals_high)]
        for duo in range(2):
            columns = pl.ds(duo * 128, 128)
            query = turned(
                q_ref[rows, columns].astype(jnp.float32), cos_ref[rows, :], sin_ref[rows, :]
            ).astype(jnp.bfloat16)
            out = jnp.zeros((128, 128), jnp.float32)
            for side in range(2):
                head = 2 * duo + side
                scores = lax.dot_general(
                    query, keys_of[side], contract, preferred_element_type=jnp.float32
                ) * HD ** (-0.5)
                exponent = jnp.where(keep, jnp.exp(scores), 0.0)
                denominator = jnp.sum(exponent, axis=1, keepdims=True) + jnp.exp(
                    aux_ref[4 + head : 5 + head, 0:1]
                )
                probs = (exponent / denominator).astype(jnp.bfloat16)
                out = out + jnp.dot(probs, vals_of[side], preferred_element_type=jnp.float32)
            out = out.astype(jnp.bfloat16)
            for piece in range(4):
                row = block * W + piece * 32
                attended[row // ROWS, row % ROWS : row % ROWS + 32, duo * 128 : duo * 128 + 128] = (
                    out[piece * 32 : piece * 32 + 32]
                )

    swaps = []
    for step, device in zip((1, 2, 3), mates(s, t)):
        swaps.append(
            remote(
                attended.at[device[1]],
                heads.at[t],
                head_sem.at[0, step],
                head_sem.at[1, step],
                device,
            )
        )
    heads[t] = attended[t]
    move(2)
    for load in loads[3:]:
        load.wait()

    expert = routes_ref[...]
    column = lax.shift_right_logical(expert, 1)
    code = (((lax.shift_right_logical(column, 2) - z) & 7) * NX) + ((column - x) & 3)
    rank = jnp.zeros_like(code)
    for index, (dz, dx) in enumerate(OFFSETS):
        rank = jnp.where(code == dz * NX + dx, index, rank)
    rank = rank + jnp.where((expert & 1) == lax.rem(t, 2), 0, NCOL)
    weight = jnp.exp(logits_ref[...])
    weight = weight / jnp.sum(weight, axis=0, keepdims=True)
    spot = lax.broadcasted_iota(jnp.int32, (2 * NCOL, ROWS), 0)
    named = jnp.zeros((2 * NCOL, ROWS), jnp.float32)
    share = jnp.zeros((2 * NCOL, ROWS), jnp.float32)
    for choice in range(TOPK):
        hit = spot == rank[choice : choice + 1, :]
        named = jnp.where(hit, 1.0, named)
        share = jnp.where(hit, weight[choice : choice + 1, :], share)
    earlier = (
        lax.broadcasted_iota(jnp.int32, (ROWS, ROWS), 0)
        <= lax.broadcasted_iota(jnp.int32, (ROWS, ROWS), 1)
    ).astype(jnp.float32)
    counted = named * jnp.dot(
        named.astype(jnp.bfloat16),
        earlier.astype(jnp.bfloat16),
        preferred_element_type=jnp.float32,
    )
    widen = (
        lax.shift_right_logical(lax.broadcasted_iota(jnp.int32, (SLOTS, 2 * NCOL), 0), 3)
        == lax.broadcasted_iota(jnp.int32, (SLOTS, 2 * NCOL), 1)
    ).astype(jnp.float32)
    widen = widen.astype(jnp.bfloat16)
    number = (lax.broadcasted_iota(jnp.int32, (SLOTS, ROWS), 0) & 7) + 1
    picks = (
        jnp.dot(widen, counted.astype(jnp.bfloat16), preferred_element_type=jnp.float32)
        == number.astype(jnp.float32)
    )
    share_high = share.astype(jnp.bfloat16)
    share_low = (share - share_high.astype(jnp.float32)).astype(jnp.bfloat16)
    for part, target in ((share_high, coarse_ref), (share_low, fine_ref)):
        wide = jnp.dot(widen, part, preferred_element_type=jnp.float32)
        target[...] = jnp.where(picks, wide, 0.0).astype(jnp.bfloat16)
    picks_buf[...] = jnp.where(picks, 1.0, 0.0).astype(jnp.bfloat16)

    for swap in swaps:
        swap.wait_recv()

    @pl.loop(0, D // 512)
    def _(tile):
        columns = pl.ds(pl.multiple_of(tile * 512, 512), 512)
        total = jnp.zeros((ROWS, 512), jnp.float32)
        for source in range(NT):
            total = total + jnp.dot(
                heads[source],
                wo_buf[source * 256 : source * 256 + 256, columns],
                preferred_element_type=jnp.float32,
            )
        after_ref[:, columns] = total

    @pl.loop(0, ROWS // 16)
    def _(tile):
        rows = pl.ds(pl.multiple_of(tile * 16, 16), 16)
        value = rms_scale(after_ref[rows, :]) * mix_ref[...]
        value = res_ref[rows, :].astype(jnp.float32) + value
        after_ref[rows, :] = value
        normed[rows, :] = (rms_scale(value) * ffn_ref[...]).astype(jnp.bfloat16)

    @pl.loop(0, D // TILE)
    def _(tile):
        columns = pl.ds(pl.multiple_of(tile * TILE, TILE), TILE)
        outgoing_ref[:, columns] = jnp.dot(
            picks_buf[...], normed[:, columns], preferred_element_type=jnp.float32
        ).astype(jnp.bfloat16)

    trades = []
    for which, target in enumerate((gate_out, up_out, down_out)):
        for side in range(2):
            moves[which, side].wait_recv()
            trades.append(
                remote(
                    target.at[2 + side],
                    target.at[side],
                    swap_sem.at[0, which, side],
                    swap_sem.at[1, which, side],
                    sibling,
                )
            )
    for copy in trades:
        copy.wait()
    for copy in list(moves.values()) + halos + swaps:
        copy.wait_send()


def attend(*arrays):
    vmem = pl.BlockSpec(memory_space=pltpu.VMEM)
    hbm = pl.BlockSpec(memory_space=pltpu.HBM)
    dma = pltpu.SemaphoreType.DMA
    bf16 = jnp.bfloat16
    return pl.pallas_call(
        attention_kernel,
        out_shape=(
            jax.ShapeDtypeStruct((ROWS, D), jnp.float32),
            jax.ShapeDtypeStruct((SLOTS, D), bf16),
            jax.ShapeDtypeStruct((SLOTS, ROWS), bf16),
            jax.ShapeDtypeStruct((SLOTS, ROWS), bf16),
            jax.ShapeDtypeStruct((4, D, TILE), bf16),
            jax.ShapeDtypeStruct((4, D, TILE), bf16),
            jax.ShapeDtypeStruct((4, TILE, D), bf16),
        ),
        in_specs=[vmem] * 3 + [hbm] * 12,
        out_specs=(vmem,) * 4 + (hbm,) * 3,
        scratch_shapes=[
            pltpu.VMEM((SPAN, 256), bf16),
            pltpu.VMEM((2 * HD, SPAN), bf16),
            pltpu.VMEM((1024, D), bf16),
            pltpu.VMEM((ROWS, D), bf16),
            pltpu.VMEM((1, D), jnp.float32),
            pltpu.VMEM((1, D), jnp.float32),
            pltpu.VMEM((TOPK, ROWS), jnp.int32),
            pltpu.VMEM((TOPK, ROWS), jnp.float32),
            pltpu.VMEM((5, W, 128), bf16),
            pltpu.VMEM((5, 1, 128), jnp.float32),
            pltpu.VMEM((NT, ROWS, 256), bf16),
            pltpu.VMEM((NT, ROWS, 256), bf16),
            pltpu.VMEM((ROWS, D), bf16),
            pltpu.VMEM((SLOTS, ROWS), bf16),
            dma((9,)),
            dma((2, 4)),
            dma((2, 4)),
            dma((2, 3, 2)),
            dma((2, 3, 2)),
        ],
        compiler_params=pltpu.CompilerParams(
            collective_id=2, has_side_effects=True, vmem_limit_bytes=60 << 20
        ),
        cost_estimate=pl.CostEstimate(
            flops=1_000_000_000, bytes_accessed=100_000_000, transcendentals=0
        ),
    )(*arrays)


def dispatch_kernel(out_ref, in_ref, transit, send_sem, recv_sem, own_sem, far_sem):
    s, t, core, z, x = place()
    near, far, back = mates(s, t)
    greet(partners_of(s, t, core, z, x))
    arrived = {}
    for index, (dz, dx) in enumerate(OFFSETS):
        for kind in range(2):
            target = in_ref.at[0, index] if kind == 0 else transit.at[index]
            if index == SELF:
                copy = pltpu.make_async_copy(out_ref.at[kind, index], target, own_sem.at[kind])
                copy.start()
            else:
                copy = remote(
                    out_ref.at[kind, index],
                    target,
                    send_sem.at[kind, index],
                    recv_sem.at[kind, index],
                    (shifted(z, x, core, dz, dx), t),
                )
            arrived[kind, index] = copy
    forwards = []
    for group in range(GROUPS):
        block = pl.ds(group * GROUP, GROUP)
        for kind in range(2):
            for index in range(group * GROUP, (group + 1) * GROUP):
                if index == SELF:
                    arrived[kind, index].wait()
                else:
                    arrived[kind, index].wait_recv()
            if kind == 0:
                routes = ((in_ref.at[0, block], 1, far),)
            else:
                routes = ((transit.at[block], 3, near), (transit.at[block], 2, back))
            for source, slot, device in routes:
                forwards.append(
                    remote(
                        source,
                        in_ref.at[slot, block],
                        far_sem.at[0, slot, group],
                        far_sem.at[1, slot, group],
                        device,
                    )
                )
    for (kind, index), copy in arrived.items():
        if index != SELF:
            copy.wait_send()
    for copy in forwards:
        copy.wait()


def dispatch(outgoing):
    return pl.pallas_call(
        dispatch_kernel,
        out_shape=jax.ShapeDtypeStruct((4, NCOL, CAP, D), jnp.bfloat16),
        in_specs=[pl.BlockSpec(memory_space=pltpu.VMEM)],
        out_specs=pl.BlockSpec(memory_space=pl.ANY),
        scratch_shapes=[
            pltpu.VMEM((NCOL, CAP, D), jnp.bfloat16),
            pltpu.SemaphoreType.DMA((2, NCOL)),
            pltpu.SemaphoreType.DMA((2, NCOL)),
            pltpu.SemaphoreType.DMA((2,)),
            pltpu.SemaphoreType.DMA((2, 4, GROUPS)),
        ],
        compiler_params=pltpu.CompilerParams(
            collective_id=0, has_side_effects=True, vmem_limit_bytes=58 << 20
        ),
        cost_estimate=pl.CostEstimate(flops=0, bytes_accessed=150_000_000, transcendentals=0),
    )(outgoing)


def expert_kernel(
    rows_ref,
    gate_hbm,
    up_hbm,
    down_hbm,
    ret_ref,
    gate_ref,
    up_ref,
    down_ref,
    block_rows,
    hidden,
    mine,
    away,
    theirs,
    total,
    load_sem,
    pair_sem,
    send_sem,
    recv_sem,
):
    s, t, core, z, x = place()
    near, far, back = mates(s, t)
    loads = [
        pltpu.make_async_copy(source, target, load_sem.at[number])
        for number, (source, target) in enumerate(
            ((gate_hbm, gate_ref), (up_hbm, up_ref), (down_hbm, down_ref))
        )
    ]
    for load in loads:
        load.start()
    greet(partners_of(s, t, core, z, x))
    for load in loads:
        load.wait()
    count = 4 * GROUP * CAP
    pairs = {}
    sends = []
    own = []

    def compute(group):
        block = pl.ds(group * GROUP, GROUP)
        block_rows[...] = (
            rows_ref[:, block].astype(jnp.float32).reshape(count, D).astype(jnp.bfloat16)
        )

        @pl.loop(0, 4)
        def _(part):
            gate_pre = jnp.dot(block_rows[...], gate_ref[part], preferred_element_type=jnp.float32)
            up_pre = jnp.dot(block_rows[...], up_ref[part], preferred_element_type=jnp.float32)
            gated = jnp.minimum(gate_pre, 7.0)
            upper = jnp.clip(up_pre, -7.0, 7.0)
            value = (upper + 1.0) * gated * jax.nn.sigmoid(1.702 * gated)
            hidden[part] = value.astype(jnp.bfloat16)

        @pl.loop(0, D // TILE)
        def _(column):
            columns = pl.ds(pl.multiple_of(column * TILE, TILE), TILE)
            term = jnp.zeros((count, TILE), jnp.float32)
            for part in range(4):
                term = term + jnp.dot(
                    hidden[part], down_ref[part, :, columns], preferred_element_type=jnp.float32
                )
            term = term.reshape(4, GROUP, CAP, TILE).astype(jnp.bfloat16)
            mine[block, :, columns] = term[0]
            away[:, block, :, columns] = term[1:]

    def swap(group):
        block = pl.ds(group * GROUP, GROUP)
        for source, slot, device in ((1, 1, near), (2, 2, back), (0, 0, far)):
            pairs[slot, group] = remote(
                away.at[source, block],
                theirs.at[slot, block],
                pair_sem.at[0, slot, group],
                pair_sem.at[1, slot, group],
                device,
            )

    def add(group):
        block = pl.ds(group * GROUP, GROUP)
        for slot in range(3):
            pairs[slot, group].wait_recv()
        total[1, block] = (
            theirs[1, block].astype(jnp.float32) + theirs[2, block].astype(jnp.float32)
        ).astype(jnp.bfloat16)
        total[0, block] = (
            mine[block].astype(jnp.float32) + theirs[0, block].astype(jnp.float32)
        ).astype(jnp.bfloat16)

    def home(group):
        for kind in (1, 0):
            for index in range(group * GROUP, (group + 1) * GROUP):
                dz, dx = OFFSETS[index]
                if index == SELF:
                    copy = pltpu.make_async_copy(
                        total.at[kind, index], ret_ref.at[kind, index], send_sem.at[kind, index]
                    )
                    copy.start()
                    own.append(copy)
                else:
                    sends.append(
                        remote(
                            total.at[kind, index],
                            ret_ref.at[kind, index],
                            send_sem.at[kind, index],
                            recv_sem.at[kind, index],
                            (shifted(z, x, core, NZ - dz, NX - dx), t),
                        )
                    )

    behind = 2
    for step in range(GROUPS + behind):
        if step < GROUPS:
            compute(BACK[step])
        if step >= behind:
            add(BACK[step - behind])
        if step < GROUPS:
            swap(BACK[step])
        if step >= behind:
            home(BACK[step - behind])
    for copy in pairs.values():
        copy.wait_send()
    for copy in own:
        copy.wait()
    for copy in sends:
        copy.wait()


def expert_outputs(rows_in, gate, up, down):
    half = (2, NCOL, CAP, D)
    third = (3, NCOL, CAP, D)
    count = 4 * GROUP * CAP
    vmem = pl.BlockSpec(memory_space=pltpu.VMEM)
    return pl.pallas_call(
        expert_kernel,
        out_shape=jax.ShapeDtypeStruct(half, jnp.bfloat16),
        in_specs=[vmem] + [pl.BlockSpec(memory_space=pltpu.HBM)] * 3,
        out_specs=pl.BlockSpec(memory_space=pl.ANY),
        scratch_shapes=[
            pltpu.VMEM((4, D, TILE), jnp.bfloat16),
            pltpu.VMEM((4, D, TILE), jnp.bfloat16),
            pltpu.VMEM((4, TILE, D), jnp.bfloat16),
            pltpu.VMEM((count, D), jnp.bfloat16),
            pltpu.VMEM((4, count, TILE), jnp.bfloat16),
            pltpu.VMEM((NCOL, CAP, D), jnp.bfloat16),
            pltpu.VMEM(third, jnp.bfloat16),
            pltpu.VMEM(third, jnp.bfloat16),
            pltpu.VMEM(half, jnp.bfloat16),
            pltpu.SemaphoreType.DMA((3,)),
            pltpu.SemaphoreType.DMA((2, 3, GROUPS)),
            pltpu.SemaphoreType.DMA((2, NCOL)),
            pltpu.SemaphoreType.DMA((2, NCOL)),
        ],
        compiler_params=pltpu.CompilerParams(
            collective_id=1, has_side_effects=True, vmem_limit_bytes=58 << 20
        ),
        cost_estimate=pl.CostEstimate(
            flops=13_000_000_000, bytes_accessed=150_000_000, transcendentals=0
        ),
    )(rows_in, gate, up, down)


def rms_scale(vector):
    return vector * lax.rsqrt(jnp.mean(vector * vector, axis=-1, keepdims=True) + 1e-06)


def body(
    residual,
    queries,
    keys,
    values,
    documents,
    sink,
    out_weight,
    mix_gain,
    ffn_gain,
    out_gain,
    routes,
    route_logits,
    gate_weight,
    up_weight,
    down_weight,
):
    positions = lax.axis_index("sp") * SPAN + jnp.arange(SPAN, dtype=jnp.int32)
    half_size = HD // 2
    lanes = jnp.arange(128, dtype=jnp.int32)
    inverse = 10000.0 ** (-(lanes % half_size).astype(jnp.float32) / half_size)
    angles = positions.astype(jnp.float32)[:, None] * inverse[None, :]
    sign = jnp.where(lanes % HD < half_size, -1.0, 1.0)
    cosine, sine = jnp.cos(angles), jnp.sin(angles) * sign[None, :]
    aux = jnp.concatenate(
        [
            documents.astype(jnp.float32).reshape(SPAN // W, W),
            jnp.zeros((1, W), jnp.float32),
            jnp.broadcast_to(sink[:, None], (4, W)),
        ],
        axis=0,
    )
    after_mix, outgoing, coarse, fine, gate, up, down = attend(
        cosine,
        sine,
        aux,
        queries,
        keys.T,
        values.T,
        out_weight,
        residual,
        mix_gain.reshape(1, D),
        ffn_gain.reshape(1, D),
        routes.T,
        route_logits.T,
        gate_weight[0],
        up_weight[0],
        down_weight[0],
    )
    rows_in = dispatch(outgoing.reshape(2, NCOL, CAP, D))
    returned = expert_outputs(rows_in, gate, up, down).reshape(SLOTS, D)
    contract = (((0,), (0,)), ((), ()))
    expert_mix = lax.dot_general(
        coarse, returned, contract, preferred_element_type=jnp.float32
    ) + lax.dot_general(fine, returned, contract, preferred_element_type=jnp.float32)
    return (after_mix + rms_scale(expert_mix) * out_gain).astype(jnp.bfloat16)


def solution(mesh):
    in_specs = (
        P(("sp", "tp"), None),
        P("sp", "tp"),
        P("sp", "tp"),
        P("sp", "tp"),
        P("sp"),
        P("tp"),
        P(),
        P(),
        P(),
        P(),
        P(("sp", "tp"), None),
        P(("sp", "tp"), None),
        P("sp", None, "tp"),
        P("sp", None, "tp"),
        P("sp", "tp", None),
    )
    out_specs = P(("sp", "tp"), None)
    return jax.shard_map(body, mesh=mesh, in_specs=in_specs, out_specs=out_specs, check_vma=False)
```

```python
import jax
import jax.numpy as jnp
from jax import lax
from jax.experimental import pallas as pl
from jax.experimental.pallas import tpu as pltpu
from jax.sharding import PartitionSpec as P

HD = 64
TOPK = 4
W = 128
D = 2048
CAP = 8
NZ, NX, NT = 8, 4, 4
NCOL = NZ * NX
MESH = pl.DeviceIdType.MESH

NEAR_Z = (1, 7, 2, 6, 3, 5)
OFFSETS = (
    ((0, 1), (0, 3))
    + tuple((dz, dx) for dx in (1, 3) for dz in NEAR_Z)
    + tuple((4, dx) for dx in (1, 3, 2, 0))
    + tuple((dz, dx) for dx in (2, 0) for dz in NEAR_Z)
    + ((0, 2), (0, 0))
)
SELF = OFFSETS.index((0, 0))
SPLIT = ((0, 2),) + tuple((start, 4) for start in range(2, 30, 4)) + ((30, 2),)
TILE = 256
ROWS = 96
SPAN = 384
SLOTS = 2 * NCOL * CAP
NS = 2 * NCOL


def place():
    s = lax.axis_index("sp")
    t = lax.axis_index("tp")
    core = lax.rem(s, 2)
    column = lax.div(s, 2)
    return s, t, core, lax.div(column, NX), lax.rem(column, NX)


def shifted(z, x, core, dz, dx):
    return (lax.rem(z + dz, NZ) * NX + lax.rem(x + dx, NX)) * 2 + core


def mates(s, t):
    return [(s, lax.rem(t + step, NT)) for step in (1, 2, 3)]


def partners_of(s, t, core, z, x):
    found = mates(s, t)
    for index, (dz, dx) in enumerate(OFFSETS):
        if index != SELF:
            found.append((shifted(z, x, core, dz, dx), t))
    return found


def remote(source, target, send_sem, recv_sem, device):
    copy = pltpu.make_async_remote_copy(
        src_ref=source,
        dst_ref=target,
        send_sem=send_sem,
        recv_sem=recv_sem,
        device_id=device,
        device_id_type=MESH,
    )
    copy.start()
    return copy


def layer_kernel(
    cos_ref,
    sin_ref,
    aux_ref,
    q_hbm,
    k_hbm,
    v_hbm,
    wo_hbm,
    res_hbm,
    mix_hbm,
    ffn_hbm,
    routes_hbm,
    logits_hbm,
    gate_hbm,
    up_hbm,
    down_hbm,
    after_ref,
    coarse_ref,
    fine_ref,
    ret_ref,
    q_ref,
    kv_ref,
    wo_buf,
    res_ref,
    mix_ref,
    ffn_ref,
    routes_ref,
    logits_ref,
    kv_ext,
    doc_ext,
    attended,
    heads,
    normed,
    picks_buf,
    out_ref,
    gate_ref,
    up_ref,
    down_ref,
    rows_ref,
    transit,
    block_rows,
    hidden,
    mine,
    away,
    theirs,
    total,
    load_sem,
    halo_sem,
    head_sem,
    move_sem,
    swap_sem,
    go_send_sem,
    go_recv_sem,
    own_sem,
    far_sem,
    pair_sem,
    send_sem,
    recv_sem,
):
    s, t, core, z, x = place()
    above = (lax.rem(s + 1, NS), t)
    below = (lax.rem(s + NS - 1, NS), t)
    sibling = (s + 1 - 2 * core, t)
    keeper = core == lax.rem(t, 2)
    barrier = pltpu.get_barrier_semaphore()
    near, far, back = mates(s, t)
    found = [above, below] + partners_of(s, t, core, z, x)
    for partner in found:
        pl.semaphore_signal(barrier, inc=1, device_id=partner, device_id_type=MESH)
    loads = [
        pltpu.make_async_copy(source, target, load_sem.at[number])
        for number, (source, target) in enumerate(
            (
                (k_hbm, kv_ref.at[pl.ds(0, HD)]),
                (v_hbm, kv_ref.at[pl.ds(HD, HD)]),
                (q_hbm, q_ref),
                (routes_hbm, routes_ref),
                (logits_hbm, logits_ref),
                (wo_hbm, wo_buf),
                (res_hbm, res_ref),
                (mix_hbm, mix_ref),
                (ffn_hbm, ffn_ref),
            )
        )
    ]
    for load in loads:
        load.start()
    pl.semaphore_wait(barrier, len(found))

    moves = {}

    def move(which):
        for side, step in ((0, 1), (1, 3)):
            neighbour = lax.rem(t + step, NT)
            half = jnp.where(keeper, side, lax.div(neighbour, 2))
            device = (jnp.where(keeper, sibling[0], s), jnp.where(keeper, t, neighbour))
            piece = pl.ds(pl.multiple_of(half * TILE, TILE), TILE)
            if which == 2:
                source, target = down_hbm.at[piece, :], down_ref.at[2 + side]
            elif which == 1:
                source, target = up_hbm.at[:, piece], up_ref.at[2 + side]
            else:
                source, target = gate_hbm.at[:, piece], gate_ref.at[2 + side]
            moves[which, side] = remote(
                source, target, move_sem.at[0, which, side], move_sem.at[1, which, side], device
            )

    move(0)
    move(1)
    for load in loads[:3]:
        load.wait()

    lane = lax.broadcasted_iota(jnp.int32, (128, 128), 1)
    low_half = (lane & 32) == 0
    left = lane < 64

    def turned(value, cosine, sine):
        swapped = jnp.where(low_half, pltpu.roll(value, 96, 1), pltpu.roll(value, 32, 1))
        return value * cosine + swapped * sine

    for block in (0, 2, 1):
        rows = pl.ds(block * W, W)
        pair = kv_ref[:, block * W : block * W + W].astype(jnp.float32).T
        key_turned = turned(pair, cos_ref[rows, :], sin_ref[rows, :])
        kv_ext[block + 1] = jnp.where(left, key_turned, pair).astype(jnp.bfloat16)
        doc_ext[block + 1] = aux_ref[block : block + 1, :]
    halos = [
        remote(kv_ext.at[1], kv_ext.at[4], halo_sem.at[0, 0], halo_sem.at[1, 0], below),
        remote(kv_ext.at[3], kv_ext.at[0], halo_sem.at[0, 1], halo_sem.at[1, 1], above),
        remote(doc_ext.at[1], doc_ext.at[4], halo_sem.at[0, 2], halo_sem.at[1, 2], below),
        remote(doc_ext.at[3], doc_ext.at[0], halo_sem.at[0, 3], halo_sem.at[1, 3], above),
    ]

    contract = (((1,), (1,)), ((), ()))
    for block in (1, 0, 2):
        if block == 0:
            for halo in halos:
                halo.wait_recv()
        rows = pl.ds(block * W, W)
        keys_low, keys_high, vals_low, vals_high, keep = [], [], [], [], []
        doc_query = jnp.broadcast_to(aux_ref[block : block + 1, :], (128, 128)).T
        for part in range(3):
            pair = kv_ext[block + part].astype(jnp.float32)
            other = pltpu.roll(pair, 64, 1)
            keys_low.append(jnp.where(left, pair, 0.0).astype(jnp.bfloat16))
            keys_high.append(jnp.where(left, 0.0, other).astype(jnp.bfloat16))
            vals_low.append(jnp.where(left, other, 0.0).astype(jnp.bfloat16))
            vals_high.append(jnp.where(left, 0.0, pair).astype(jnp.bfloat16))
            gap = (part - 1) * W + lane - lax.broadcasted_iota(jnp.int32, (128, 128), 0)
            place_of = s * SPAN + (block + part - 1) * W + lane
            doc_key = doc_ext[block + part]
            keep.append(
                (jnp.abs(gap) <= W)
                & (place_of >= 0)
                & (place_of < NS * SPAN)
                & (doc_query == doc_key)
            )
        keep = jnp.concatenate(keep, axis=1)
        keys_of = [jnp.concatenate(part, axis=0) for part in (keys_low, keys_high)]
        vals_of = [jnp.concatenate(part, axis=0) for part in (vals_low, vals_high)]
        for duo in range(2):
            columns = pl.ds(duo * 128, 128)
            query = turned(
                q_ref[rows, columns].astype(jnp.float32), cos_ref[rows, :], sin_ref[rows, :]
            ).astype(jnp.bfloat16)
            out = jnp.zeros((128, 128), jnp.float32)
            for side in range(2):
                head = 2 * duo + side
                scores = lax.dot_general(
                    query, keys_of[side], contract, preferred_element_type=jnp.float32
                ) * HD ** (-0.5)
                exponent = jnp.where(keep, jnp.exp(scores), 0.0)
                denominator = jnp.sum(exponent, axis=1, keepdims=True) + jnp.exp(
                    aux_ref[4 + head : 5 + head, 0:1]
                )
                probs = (exponent / denominator).astype(jnp.bfloat16)
                out = out + jnp.dot(probs, vals_of[side], preferred_element_type=jnp.float32)
            out = out.astype(jnp.bfloat16)
            for piece in range(4):
                row = block * W + piece * 32
                attended[row // ROWS, row % ROWS : row % ROWS + 32, duo * 128 : duo * 128 + 128] = (
                    out[piece * 32 : piece * 32 + 32]
                )

    swaps = []
    for step, device in zip((1, 2, 3), mates(s, t)):
        swaps.append(
            remote(
                attended.at[device[1]],
                heads.at[t],
                head_sem.at[0, step],
                head_sem.at[1, step],
                device,
            )
        )
    heads[t] = attended[t]
    move(2)
    for load in loads[3:]:
        load.wait()

    expert = routes_ref[...]
    column = lax.shift_right_logical(expert, 1)
    code = (((lax.shift_right_logical(column, 2) - z) & 7) * NX) + ((column - x) & 3)
    rank = jnp.zeros_like(code)
    for index, (dz, dx) in enumerate(OFFSETS):
        rank = jnp.where(code == dz * NX + dx, index, rank)
    rank = rank + jnp.where((expert & 1) == lax.rem(t, 2), 0, NCOL)
    weight = jnp.exp(logits_ref[...])
    weight = weight / jnp.sum(weight, axis=0, keepdims=True)
    spot = lax.broadcasted_iota(jnp.int32, (2 * NCOL, ROWS), 0)
    named = jnp.zeros((2 * NCOL, ROWS), jnp.float32)
    share = jnp.zeros((2 * NCOL, ROWS), jnp.float32)
    for choice in range(TOPK):
        hit = spot == rank[choice : choice + 1, :]
        named = jnp.where(hit, 1.0, named)
        share = jnp.where(hit, weight[choice : choice + 1, :], share)
    earlier = (
        lax.broadcasted_iota(jnp.int32, (ROWS, ROWS), 0)
        <= lax.broadcasted_iota(jnp.int32, (ROWS, ROWS), 1)
    ).astype(jnp.float32)
    counted = named * jnp.dot(
        named.astype(jnp.bfloat16),
        earlier.astype(jnp.bfloat16),
        preferred_element_type=jnp.float32,
    )
    widen = (
        lax.shift_right_logical(lax.broadcasted_iota(jnp.int32, (SLOTS, 2 * NCOL), 0), 3)
        == lax.broadcasted_iota(jnp.int32, (SLOTS, 2 * NCOL), 1)
    ).astype(jnp.float32)
    widen = widen.astype(jnp.bfloat16)
    number = (lax.broadcasted_iota(jnp.int32, (SLOTS, ROWS), 0) & 7) + 1
    picks = (
        jnp.dot(widen, counted.astype(jnp.bfloat16), preferred_element_type=jnp.float32)
        == number.astype(jnp.float32)
    )
    share_high = share.astype(jnp.bfloat16)
    share_low = (share - share_high.astype(jnp.float32)).astype(jnp.bfloat16)
    for part, target in ((share_high, coarse_ref), (share_low, fine_ref)):
        wide = jnp.dot(widen, part, preferred_element_type=jnp.float32)
        target[...] = jnp.where(picks, wide, 0.0).astype(jnp.bfloat16)
    picks_buf[...] = jnp.where(picks, 1.0, 0.0).astype(jnp.bfloat16)

    for swap in swaps:
        swap.wait_recv()

    @pl.loop(0, D // 512)
    def _(tile):
        columns = pl.ds(pl.multiple_of(tile * 512, 512), 512)
        total = jnp.zeros((ROWS, 512), jnp.float32)
        for source in range(NT):
            total = total + jnp.dot(
                heads[source],
                wo_buf[source * 256 : source * 256 + 256, columns],
                preferred_element_type=jnp.float32,
            )
        after_ref[:, columns] = total

    @pl.loop(0, ROWS // 16)
    def _(tile):
        rows = pl.ds(pl.multiple_of(tile * 16, 16), 16)
        value = rms_scale(after_ref[rows, :]) * mix_ref[...]
        value = res_ref[rows, :].astype(jnp.float32) + value
        after_ref[rows, :] = value
        normed[rows, :] = (rms_scale(value) * ffn_ref[...]).astype(jnp.bfloat16)

    @pl.loop(0, D // TILE)
    def _(tile):
        columns = pl.ds(pl.multiple_of(tile * TILE, TILE), TILE)
        packed = jnp.dot(picks_buf[...], normed[:, columns], preferred_element_type=jnp.float32)
        out_ref[:, :, :, columns] = packed.reshape(2, NCOL, CAP, TILE).astype(jnp.bfloat16)

    trades = []

    def trade(which):
        target = (gate_ref, up_ref, down_ref)[which]
        for side in range(2):
            moves[which, side].wait_recv()
            trades.append(
                remote(
                    target.at[2 + side],
                    target.at[side],
                    swap_sem.at[0, which, side],
                    swap_sem.at[1, which, side],
                    sibling,
                )
            )

    trade(0)
    trade(1)

    arrived, forwards, pairs, sends, own = {}, {}, {}, [], []
    for index, (dz, dx) in enumerate(OFFSETS):
        for kind in range(2):
            target = rows_ref.at[0, index] if kind == 0 else transit.at[index]
            if index == SELF:
                copy = pltpu.make_async_copy(out_ref.at[kind, index], target, own_sem.at[kind])
                copy.start()
            else:
                copy = remote(
                    out_ref.at[kind, index],
                    target,
                    go_send_sem.at[kind, index],
                    go_recv_sem.at[kind, index],
                    (shifted(z, x, core, dz, dx), t),
                )
            arrived[kind, index] = copy

    def forward(group):
        start, size = SPLIT[group]
        block = pl.ds(start, size)
        for kind in range(2):
            for index in range(start, start + size):
                if index == SELF:
                    arrived[kind, index].wait()
                else:
                    arrived[kind, index].wait_recv()
            if kind == 0:
                routes = ((rows_ref.at[0, block], 1, far),)
            else:
                routes = ((transit.at[block], 3, near), (transit.at[block], 2, back))
            for source, slot, device in routes:
                forwards[slot, group] = remote(
                    source,
                    rows_ref.at[slot, block],
                    far_sem.at[0, slot - 1, group],
                    far_sem.at[1, slot - 1, group],
                    device,
                )

    def compute(group):
        start, size = SPLIT[group]
        block = pl.ds(start, size)
        count = 4 * size * CAP
        for slot in (1, 2, 3):
            forwards[slot, group].wait_recv()
        block_rows[:count] = (
            rows_ref[:, block].astype(jnp.float32).reshape(count, D).astype(jnp.bfloat16)
        )

        @pl.loop(0, 4)
        def _(part):
            gate_pre = jnp.dot(
                block_rows[:count], gate_ref[part], preferred_element_type=jnp.float32
            )
            up_pre = jnp.dot(block_rows[:count], up_ref[part], preferred_element_type=jnp.float32)
            gated = jnp.minimum(gate_pre, 7.0)
            upper = jnp.clip(up_pre, -7.0, 7.0)
            value = (upper + 1.0) * gated * jax.nn.sigmoid(1.702 * gated)
            hidden[part, :count] = value.astype(jnp.bfloat16)

        @pl.loop(0, D // TILE)
        def _(column):
            columns = pl.ds(pl.multiple_of(column * TILE, TILE), TILE)
            term = jnp.zeros((count, TILE), jnp.float32)
            for part in range(4):
                term = term + jnp.dot(
                    hidden[part, :count],
                    down_ref[part, :, columns],
                    preferred_element_type=jnp.float32,
                )
            term = term.reshape(4, size, CAP, TILE).astype(jnp.bfloat16)
            mine[block, :, columns] = term[0]
            away[:, block, :, columns] = term[1:]

    def swap(group):
        start, size = SPLIT[group]
        block = pl.ds(start, size)
        for source, slot, device in ((1, 1, near), (2, 2, back), (0, 0, far)):
            pairs[slot, group] = remote(
                away.at[source, block],
                theirs.at[slot, block],
                pair_sem.at[0, slot, group],
                pair_sem.at[1, slot, group],
                device,
            )

    def add(group):
        start, size = SPLIT[group]
        block = pl.ds(start, size)
        for slot in range(3):
            pairs[slot, group].wait_recv()
        total[1, block] = (
            theirs[1, block].astype(jnp.float32) + theirs[2, block].astype(jnp.float32)
        ).astype(jnp.bfloat16)
        total[0, block] = (
            mine[block].astype(jnp.float32) + theirs[0, block].astype(jnp.float32)
        ).astype(jnp.bfloat16)

    def home(group):
        start, size = SPLIT[group]
        for kind in (1, 0):
            for index in range(start, start + size):
                dz, dx = OFFSETS[index]
                if index == SELF:
                    copy = pltpu.make_async_copy(
                        total.at[kind, index], ret_ref.at[kind, index], send_sem.at[kind, index]
                    )
                    copy.start()
                    own.append(copy)
                else:
                    sends.append(
                        remote(
                            total.at[kind, index],
                            ret_ref.at[kind, index],
                            send_sem.at[kind, index],
                            recv_sem.at[kind, index],
                            (shifted(z, x, core, NZ - dz, NX - dx), t),
                        )
                    )

    last = len(SPLIT)
    for step in range(last + 3):
        if step < last:
            forward(step)
        if step == 0:
            trade(2)
        if step == 1:
            for copy in trades:
                copy.wait_recv()
        if 1 <= step <= last:
            compute(step - 1)
        if step >= 3:
            add(step - 3)
        if 1 <= step <= last:
            swap(step - 1)
        if step >= 3:
            home(step - 3)
    for (kind, index), copy in arrived.items():
        if index != SELF:
            copy.wait_send()
    for copy in list(forwards.values()) + list(pairs.values()) + trades:
        copy.wait_send()
    for copy in list(moves.values()) + halos + swaps:
        copy.wait_send()
    for copy in own:
        copy.wait()
    for copy in sends:
        copy.wait()


def layer(*arrays):
    vmem = pl.BlockSpec(memory_space=pltpu.VMEM)
    hbm = pl.BlockSpec(memory_space=pltpu.HBM)
    dma = pltpu.SemaphoreType.DMA
    bf16 = jnp.bfloat16
    half = (2, NCOL, CAP, D)
    third = (3, NCOL, CAP, D)
    count = 4 * max(size for _, size in SPLIT) * CAP
    return pl.pallas_call(
        layer_kernel,
        out_shape=(
            jax.ShapeDtypeStruct((ROWS, D), jnp.float32),
            jax.ShapeDtypeStruct((SLOTS, ROWS), bf16),
            jax.ShapeDtypeStruct((SLOTS, ROWS), bf16),
            jax.ShapeDtypeStruct(half, bf16),
        ),
        in_specs=[vmem] * 3 + [hbm] * 12,
        out_specs=(vmem,) * 3 + (hbm,),
        scratch_shapes=[
            pltpu.VMEM((SPAN, 256), bf16),
            pltpu.VMEM((2 * HD, SPAN), bf16),
            pltpu.VMEM((1024, D), bf16),
            pltpu.VMEM((ROWS, D), bf16),
            pltpu.VMEM((1, D), jnp.float32),
            pltpu.VMEM((1, D), jnp.float32),
            pltpu.VMEM((TOPK, ROWS), jnp.int32),
            pltpu.VMEM((TOPK, ROWS), jnp.float32),
            pltpu.VMEM((5, W, 128), bf16),
            pltpu.VMEM((5, 1, 128), jnp.float32),
            pltpu.VMEM((NT, ROWS, 256), bf16),
            pltpu.VMEM((NT, ROWS, 256), bf16),
            pltpu.VMEM((ROWS, D), bf16),
            pltpu.VMEM((SLOTS, ROWS), bf16),
            pltpu.VMEM(half, bf16),
            pltpu.VMEM((4, D, TILE), bf16),
            pltpu.VMEM((4, D, TILE), bf16),
            pltpu.VMEM((4, TILE, D), bf16),
            pltpu.VMEM((4, NCOL, CAP, D), bf16),
            pltpu.VMEM((NCOL, CAP, D), bf16),
            pltpu.VMEM((count, D), bf16),
            pltpu.VMEM((4, count, TILE), bf16),
            pltpu.VMEM((NCOL, CAP, D), bf16),
            pltpu.VMEM(third, bf16),
            pltpu.VMEM(third, bf16),
            pltpu.VMEM(half, bf16),
            dma((9,)),
            dma((2, 4)),
            dma((2, 4)),
            dma((2, 3, 2)),
            dma((2, 3, 2)),
            dma((2, NCOL)),
            dma((2, NCOL)),
            dma((2,)),
            dma((2, 3, len(SPLIT))),
            dma((2, 3, len(SPLIT))),
            dma((2, NCOL)),
            dma((2, NCOL)),
        ],
        compiler_params=pltpu.CompilerParams(
            collective_id=0, has_side_effects=True, vmem_limit_bytes=60 << 20
        ),
        cost_estimate=pl.CostEstimate(
            flops=14_000_000_000, bytes_accessed=300_000_000, transcendentals=0
        ),
    )(*arrays)


def rms_scale(vector):
    return vector * lax.rsqrt(jnp.mean(vector * vector, axis=-1, keepdims=True) + 1e-06)


def body(
    residual,
    queries,
    keys,
    values,
    documents,
    sink,
    out_weight,
    mix_gain,
    ffn_gain,
    out_gain,
    routes,
    route_logits,
    gate_weight,
    up_weight,
    down_weight,
):
    positions = lax.axis_index("sp") * SPAN + jnp.arange(SPAN, dtype=jnp.int32)
    half_size = HD // 2
    lanes = jnp.arange(128, dtype=jnp.int32)
    inverse = 10000.0 ** (-(lanes % half_size).astype(jnp.float32) / half_size)
    angles = positions.astype(jnp.float32)[:, None] * inverse[None, :]
    sign = jnp.where(lanes % HD < half_size, -1.0, 1.0)
    cosine, sine = jnp.cos(angles), jnp.sin(angles) * sign[None, :]
    aux = jnp.concatenate(
        [
            documents.astype(jnp.float32).reshape(SPAN // W, W),
            jnp.zeros((1, W), jnp.float32),
            jnp.broadcast_to(sink[:, None], (4, W)),
        ],
        axis=0,
    )
    after_mix, coarse, fine, returned = layer(
        cosine,
        sine,
        aux,
        queries,
        keys.T,
        values.T,
        out_weight,
        residual,
        mix_gain.reshape(1, D),
        ffn_gain.reshape(1, D),
        routes.T,
        route_logits.T,
        gate_weight[0],
        up_weight[0],
        down_weight[0],
    )
    returned = returned.reshape(SLOTS, D)
    contract = (((0,), (0,)), ((), ()))
    expert_mix = lax.dot_general(
        coarse, returned, contract, preferred_element_type=jnp.float32
    ) + lax.dot_general(fine, returned, contract, preferred_element_type=jnp.float32)
    return (after_mix + rms_scale(expert_mix) * out_gain).astype(jnp.bfloat16)


def solution(mesh):
    in_specs = (
        P(("sp", "tp"), None),
        P("sp", "tp"),
        P("sp", "tp"),
        P("sp", "tp"),
        P("sp"),
        P("tp"),
        P(),
        P(),
        P(),
        P(),
        P(("sp", "tp"), None),
        P(("sp", "tp"), None),
        P("sp", None, "tp"),
        P("sp", None, "tp"),
        P("sp", "tp", None),
    )
    out_specs = P(("sp", "tp"), None)
    return jax.shard_map(body, mesh=mesh, in_specs=in_specs, out_specs=out_specs, check_vma=False)
```

```python
import jax
import jax.numpy as jnp
from jax import lax
from jax.experimental import pallas as pl
from jax.experimental.pallas import tpu as pltpu
from jax.sharding import PartitionSpec as P

HD = 64
TOPK = 4
W = 128
D = 2048
CAP = 8
NZ, NX, NT = 8, 4, 4
NCOL = NZ * NX
MESH = pl.DeviceIdType.MESH

NEAR_Z = (1, 7, 2, 6, 3, 5)
OFFSETS = (
    ((0, 1), (0, 3))
    + tuple((dz, dx) for dx in (1, 3) for dz in NEAR_Z)
    + tuple((4, dx) for dx in (1, 3, 2, 0))
    + tuple((dz, dx) for dx in (2, 0) for dz in NEAR_Z)
    + ((0, 2), (0, 0))
)
SELF = OFFSETS.index((0, 0))
SPLIT = ((0, 2),) + tuple((start, 4) for start in range(2, 30, 4)) + ((30, 2),)
TILE = 256
ROWS = 96
SPAN = 384
SLOTS = 2 * NCOL * CAP
NS = 2 * NCOL


def place():
    s = lax.axis_index("sp")
    t = lax.axis_index("tp")
    core = lax.rem(s, 2)
    column = lax.div(s, 2)
    return s, t, core, lax.div(column, NX), lax.rem(column, NX)


def shifted(z, x, core, dz, dx):
    return (lax.rem(z + dz, NZ) * NX + lax.rem(x + dx, NX)) * 2 + core


def mates(s, t):
    return [(s, lax.rem(t + step, NT)) for step in (1, 2, 3)]


def partners_of(s, t, core, z, x):
    found = mates(s, t)
    for index, (dz, dx) in enumerate(OFFSETS):
        if index != SELF:
            found.append((shifted(z, x, core, dz, dx), t))
    return found


def remote(source, target, send_sem, recv_sem, device):
    copy = pltpu.make_async_remote_copy(
        src_ref=source,
        dst_ref=target,
        send_sem=send_sem,
        recv_sem=recv_sem,
        device_id=device,
        device_id_type=MESH,
    )
    copy.start()
    return copy


def layer_kernel(
    cos_ref,
    sin_ref,
    doc_hbm,
    sink_hbm,
    q_hbm,
    k_hbm,
    v_hbm,
    wo_hbm,
    res_hbm,
    mix_hbm,
    ffn_hbm,
    routes_hbm,
    logits_hbm,
    gate_hbm,
    up_hbm,
    down_hbm,
    after_ref,
    coarse_ref,
    fine_ref,
    ret_ref,
    q_ref,
    kv_ref,
    wo_buf,
    res_ref,
    mix_ref,
    ffn_ref,
    routes_ref,
    logits_ref,
    sink_ref,
    kv_ext,
    doc_ext,
    attended,
    heads,
    normed,
    picks_buf,
    out_ref,
    gate_ref,
    up_ref,
    down_ref,
    rows_ref,
    transit,
    block_rows,
    hidden,
    mine,
    away,
    theirs,
    total,
    load_sem,
    halo_sem,
    head_sem,
    move_sem,
    swap_sem,
    go_send_sem,
    go_recv_sem,
    own_sem,
    far_sem,
    pair_sem,
    send_sem,
    recv_sem,
):
    s, t, core, z, x = place()
    above = (lax.rem(s + 1, NS), t)
    below = (lax.rem(s + NS - 1, NS), t)
    sibling = (s + 1 - 2 * core, t)
    keeper = core == lax.rem(t, 2)
    barrier = pltpu.get_barrier_semaphore()
    near, far, back = mates(s, t)
    found = [above, below] + partners_of(s, t, core, z, x)
    for partner in found:
        pl.semaphore_signal(barrier, inc=1, device_id=partner, device_id_type=MESH)
    loads = [
        pltpu.make_async_copy(source, target, load_sem.at[number])
        for number, (source, target) in enumerate(
            (
                (k_hbm, kv_ref.at[pl.ds(0, HD)]),
                (v_hbm, kv_ref.at[pl.ds(HD, HD)]),
                (q_hbm, q_ref),
                (sink_hbm, sink_ref),
                (doc_hbm.at[pl.ds(0, W)], doc_ext.at[1, 0]),
                (doc_hbm.at[pl.ds(W, W)], doc_ext.at[2, 0]),
                (doc_hbm.at[pl.ds(2 * W, W)], doc_ext.at[3, 0]),
                (routes_hbm, routes_ref),
                (logits_hbm, logits_ref),
                (wo_hbm, wo_buf),
                (res_hbm, res_ref),
                (mix_hbm, mix_ref),
                (ffn_hbm, ffn_ref),
            )
        )
    ]
    for load in loads:
        load.start()
    pl.semaphore_wait(barrier, len(found))

    moves = {}

    def move(which):
        for side, step in ((0, 1), (1, 3)):
            neighbour = lax.rem(t + step, NT)
            half = jnp.where(keeper, side, lax.div(neighbour, 2))
            device = (jnp.where(keeper, sibling[0], s), jnp.where(keeper, t, neighbour))
            piece = pl.ds(pl.multiple_of(half * TILE, TILE), TILE)
            if which == 2:
                source, target = down_hbm.at[piece, :], down_ref.at[2 + side]
            elif which == 1:
                source, target = up_hbm.at[:, piece], up_ref.at[2 + side]
            else:
                source, target = gate_hbm.at[:, piece], gate_ref.at[2 + side]
            moves[which, side] = remote(
                source, target, move_sem.at[0, which, side], move_sem.at[1, which, side], device
            )

    move(0)
    for load in loads[:7]:
        load.wait()

    lane = lax.broadcasted_iota(jnp.int32, (128, 128), 1)
    low_half = (lane & 32) == 0
    left = lane < 64

    def turned(value, cosine, sine):
        swapped = jnp.where(low_half, pltpu.roll(value, 96, 1), pltpu.roll(value, 32, 1))
        return value * cosine + swapped * sine

    for block in (0, 2, 1):
        rows = pl.ds(block * W, W)
        pair = kv_ref[:, block * W : block * W + W].astype(jnp.float32).T
        key_turned = turned(pair, cos_ref[rows, :], sin_ref[rows, :])
        kv_ext[block + 1] = jnp.where(left, key_turned, pair).astype(jnp.bfloat16)
    halos = [
        remote(kv_ext.at[1], kv_ext.at[4], halo_sem.at[0, 0], halo_sem.at[1, 0], below),
        remote(kv_ext.at[3], kv_ext.at[0], halo_sem.at[0, 1], halo_sem.at[1, 1], above),
        remote(doc_ext.at[1], doc_ext.at[4], halo_sem.at[0, 2], halo_sem.at[1, 2], below),
        remote(doc_ext.at[3], doc_ext.at[0], halo_sem.at[0, 3], halo_sem.at[1, 3], above),
    ]

    contract = (((1,), (1,)), ((), ()))
    for block in (1, 0, 2):
        if block == 0:
            for halo in halos:
                halo.wait_recv()
        rows = pl.ds(block * W, W)
        keys_low, keys_high, vals_low, vals_high, keep = [], [], [], [], []
        doc_query = jnp.broadcast_to(doc_ext[block + 1].astype(jnp.float32), (128, 128)).T
        for part in range(3):
            pair = kv_ext[block + part].astype(jnp.float32)
            other = pltpu.roll(pair, 64, 1)
            keys_low.append(jnp.where(left, pair, 0.0).astype(jnp.bfloat16))
            keys_high.append(jnp.where(left, 0.0, other).astype(jnp.bfloat16))
            vals_low.append(jnp.where(left, other, 0.0).astype(jnp.bfloat16))
            vals_high.append(jnp.where(left, 0.0, pair).astype(jnp.bfloat16))
            gap = (part - 1) * W + lane - lax.broadcasted_iota(jnp.int32, (128, 128), 0)
            place_of = s * SPAN + (block + part - 1) * W + lane
            doc_key = doc_ext[block + part].astype(jnp.float32)
            keep.append(
                (jnp.abs(gap) <= W)
                & (place_of >= 0)
                & (place_of < NS * SPAN)
                & (doc_query == doc_key)
            )
        keep = jnp.concatenate(keep, axis=1)
        keys_of = [jnp.concatenate(part, axis=0) for part in (keys_low, keys_high)]
        vals_of = [jnp.concatenate(part, axis=0) for part in (vals_low, vals_high)]
        for duo in range(2):
            columns = pl.ds(duo * 128, 128)
            query = turned(
                q_ref[rows, columns].astype(jnp.float32), cos_ref[rows, :], sin_ref[rows, :]
            ).astype(jnp.bfloat16) * HD ** (-0.5)
            out = jnp.zeros((128, 128), jnp.float32)
            for side in range(2):
                head = 2 * duo + side
                scores = lax.dot_general(
                    query, keys_of[side], contract, preferred_element_type=jnp.float32
                )
                exponent = jnp.where(keep, jnp.exp(scores), 0.0)
                denominator = jnp.sum(exponent, axis=1, keepdims=True) + jnp.exp(
                    jnp.full((1, 1), sink_ref[head], jnp.float32)
                )
                probs = (exponent * (1.0 / denominator)).astype(jnp.bfloat16)
                out = out + jnp.dot(probs, vals_of[side], preferred_element_type=jnp.float32)
            out = out.astype(jnp.bfloat16)
            for piece in range(4):
                row = block * W + piece * 32
                attended[row // ROWS, row % ROWS : row % ROWS + 32, duo * 128 : duo * 128 + 128] = (
                    out[piece * 32 : piece * 32 + 32]
                )

    swaps = []
    for step, device in zip((1, 2, 3), mates(s, t)):
        swaps.append(
            remote(
                attended.at[device[1]],
                heads.at[t],
                head_sem.at[0, step],
                head_sem.at[1, step],
                device,
            )
        )
    heads[t] = attended[t]
    move(1)
    move(2)
    for load in loads[7:]:
        load.wait()

    expert = routes_ref[...]
    column = lax.shift_right_logical(expert, 1)
    code = (((lax.shift_right_logical(column, 2) - z) & 7) * NX) + ((column - x) & 3)
    rank = jnp.zeros_like(code)
    for index, (dz, dx) in enumerate(OFFSETS):
        rank = jnp.where(code == dz * NX + dx, index, rank)
    rank = rank + jnp.where((expert & 1) == lax.rem(t, 2), 0, NCOL)
    weight = jnp.exp(logits_ref[...])
    weight = weight / jnp.sum(weight, axis=0, keepdims=True)
    spot = lax.broadcasted_iota(jnp.int32, (2 * NCOL, ROWS), 0)
    named = jnp.zeros((2 * NCOL, ROWS), jnp.float32)
    share = jnp.zeros((2 * NCOL, ROWS), jnp.float32)
    for choice in range(TOPK):
        hit = spot == rank[choice : choice + 1, :]
        named = jnp.where(hit, 1.0, named)
        share = jnp.where(hit, weight[choice : choice + 1, :], share)
    earlier = (
        lax.broadcasted_iota(jnp.int32, (ROWS, ROWS), 0)
        <= lax.broadcasted_iota(jnp.int32, (ROWS, ROWS), 1)
    ).astype(jnp.float32)
    counted = named * jnp.dot(
        named.astype(jnp.bfloat16),
        earlier.astype(jnp.bfloat16),
        preferred_element_type=jnp.float32,
    )
    widen = (
        lax.shift_right_logical(lax.broadcasted_iota(jnp.int32, (SLOTS, 2 * NCOL), 0), 3)
        == lax.broadcasted_iota(jnp.int32, (SLOTS, 2 * NCOL), 1)
    ).astype(jnp.float32)
    widen = widen.astype(jnp.bfloat16)
    number = (lax.broadcasted_iota(jnp.int32, (SLOTS, ROWS), 0) & 7) + 1
    picks = (
        jnp.dot(widen, counted.astype(jnp.bfloat16), preferred_element_type=jnp.float32)
        == number.astype(jnp.float32)
    )
    share_high = share.astype(jnp.bfloat16)
    share_low = (share - share_high.astype(jnp.float32)).astype(jnp.bfloat16)
    for part, target in ((share_high, coarse_ref), (share_low, fine_ref)):
        wide = jnp.dot(widen, part, preferred_element_type=jnp.float32)
        target[...] = jnp.where(picks, wide, 0.0).astype(jnp.bfloat16)
    picks_buf[...] = jnp.where(picks, 1.0, 0.0).astype(jnp.bfloat16)

    for swap in swaps:
        swap.wait_recv()

    @pl.loop(0, D // 512)
    def _(tile):
        columns = pl.ds(pl.multiple_of(tile * 512, 512), 512)
        total = jnp.zeros((ROWS, 512), jnp.float32)
        for source in range(NT):
            total = total + jnp.dot(
                heads[source],
                wo_buf[source * 256 : source * 256 + 256, columns],
                preferred_element_type=jnp.float32,
            )
        after_ref[:, columns] = total

    @pl.loop(0, ROWS // 16)
    def _(tile):
        rows = pl.ds(pl.multiple_of(tile * 16, 16), 16)
        value = rms_scale(after_ref[rows, :]) * mix_ref[...]
        value = res_ref[rows, :].astype(jnp.float32) + value
        after_ref[rows, :] = value
        normed[rows, :] = (rms_scale(value) * ffn_ref[...]).astype(jnp.bfloat16)

    @pl.loop(0, D // TILE)
    def _(tile):
        columns = pl.ds(pl.multiple_of(tile * TILE, TILE), TILE)
        packed = jnp.dot(picks_buf[...], normed[:, columns], preferred_element_type=jnp.float32)
        out_ref[:, :, :, columns] = packed.reshape(2, NCOL, CAP, TILE).astype(jnp.bfloat16)

    trades = []

    def trade(which):
        target = (gate_ref, up_ref, down_ref)[which]
        for side in range(2):
            moves[which, side].wait_recv()
            trades.append(
                remote(
                    target.at[2 + side],
                    target.at[side],
                    swap_sem.at[0, which, side],
                    swap_sem.at[1, which, side],
                    sibling,
                )
            )

    trade(0)
    trade(1)

    arrived, forwards, pairs, sends, own = {}, {}, {}, [], []
    for index, (dz, dx) in enumerate(OFFSETS):
        for kind in range(2):
            target = rows_ref.at[0, index] if kind == 0 else transit.at[index]
            if index == SELF:
                copy = pltpu.make_async_copy(out_ref.at[kind, index], target, own_sem.at[kind])
                copy.start()
            else:
                copy = remote(
                    out_ref.at[kind, index],
                    target,
                    go_send_sem.at[kind, index],
                    go_recv_sem.at[kind, index],
                    (shifted(z, x, core, dz, dx), t),
                )
            arrived[kind, index] = copy

    def forward(group):
        start, size = SPLIT[group]
        block = pl.ds(start, size)
        for kind in range(2):
            for index in range(start, start + size):
                if index == SELF:
                    arrived[kind, index].wait()
                else:
                    arrived[kind, index].wait_recv()
            if kind == 0:
                routes = ((rows_ref.at[0, block], 1, far),)
            else:
                routes = ((transit.at[block], 3, near), (transit.at[block], 2, back))
            for source, slot, device in routes:
                forwards[slot, group] = remote(
                    source,
                    rows_ref.at[slot, block],
                    far_sem.at[0, slot - 1, group],
                    far_sem.at[1, slot - 1, group],
                    device,
                )

    def compute(group):
        start, size = SPLIT[group]
        block = pl.ds(start, size)
        count = 4 * size * CAP
        for slot in (1, 2, 3):
            forwards[slot, group].wait_recv()
        block_rows[:count] = (
            rows_ref[:, block].astype(jnp.float32).reshape(count, D).astype(jnp.bfloat16)
        )

        @pl.loop(0, 4)
        def _(part):
            gate_pre = jnp.dot(
                block_rows[:count], gate_ref[part], preferred_element_type=jnp.float32
            )
            up_pre = jnp.dot(block_rows[:count], up_ref[part], preferred_element_type=jnp.float32)
            gated = jnp.minimum(gate_pre, 7.0)
            upper = jnp.clip(up_pre, -7.0, 7.0)
            value = (upper + 1.0) * gated * jax.nn.sigmoid(1.702 * gated)
            hidden[part, :count] = value.astype(jnp.bfloat16)

        @pl.loop(0, D // TILE)
        def _(column):
            columns = pl.ds(pl.multiple_of(column * TILE, TILE), TILE)
            term = jnp.zeros((count, TILE), jnp.float32)
            for part in range(4):
                term = term + jnp.dot(
                    hidden[part, :count],
                    down_ref[part, :, columns],
                    preferred_element_type=jnp.float32,
                )
            term = term.reshape(4, size, CAP, TILE).astype(jnp.bfloat16)
            mine[block, :, columns] = term[0]
            away[:, block, :, columns] = term[1:]

    def swap(group):
        start, size = SPLIT[group]
        block = pl.ds(start, size)
        for source, slot, device in ((1, 1, near), (2, 2, back), (0, 0, far)):
            pairs[slot, group] = remote(
                away.at[source, block],
                theirs.at[slot, block],
                pair_sem.at[0, slot, group],
                pair_sem.at[1, slot, group],
                device,
            )

    def add(group):
        start, size = SPLIT[group]
        block = pl.ds(start, size)
        for slot in range(3):
            pairs[slot, group].wait_recv()
        total[1, block] = (
            theirs[1, block].astype(jnp.float32) + theirs[2, block].astype(jnp.float32)
        ).astype(jnp.bfloat16)
        total[0, block] = (
            mine[block].astype(jnp.float32) + theirs[0, block].astype(jnp.float32)
        ).astype(jnp.bfloat16)

    def home(group):
        start, size = SPLIT[group]
        for kind in (1, 0):
            for index in range(start, start + size):
                dz, dx = OFFSETS[index]
                if index == SELF:
                    copy = pltpu.make_async_copy(
                        total.at[kind, index], ret_ref.at[kind, index], send_sem.at[kind, index]
                    )
                    copy.start()
                    own.append(copy)
                else:
                    sends.append(
                        remote(
                            total.at[kind, index],
                            ret_ref.at[kind, index],
                            send_sem.at[kind, index],
                            recv_sem.at[kind, index],
                            (shifted(z, x, core, NZ - dz, NX - dx), t),
                        )
                    )

    last = len(SPLIT)
    for step in range(last + 2):
        if step < last:
            forward(step)
        if step == 0:
            trade(2)
        if step == 1:
            for copy in trades:
                copy.wait_recv()
        if 1 <= step <= last:
            compute(step - 1)
        if 1 <= step <= last:
            swap(step - 1)
        if step >= 2:
            add(step - 2)
            home(step - 2)
    for (kind, index), copy in arrived.items():
        if index != SELF:
            copy.wait_send()
    for copy in list(forwards.values()) + list(pairs.values()) + trades:
        copy.wait_send()
    for copy in list(moves.values()) + halos + swaps:
        copy.wait_send()
    for copy in own:
        copy.wait()
    for copy in sends:
        copy.wait()


def layer(*arrays):
    vmem = pl.BlockSpec(memory_space=pltpu.VMEM)
    hbm = pl.BlockSpec(memory_space=pltpu.HBM)
    dma = pltpu.SemaphoreType.DMA
    bf16 = jnp.bfloat16
    half = (2, NCOL, CAP, D)
    third = (3, NCOL, CAP, D)
    count = 4 * max(size for _, size in SPLIT) * CAP
    return pl.pallas_call(
        layer_kernel,
        out_shape=(
            jax.ShapeDtypeStruct((ROWS, D), jnp.float32),
            jax.ShapeDtypeStruct((SLOTS, ROWS), bf16),
            jax.ShapeDtypeStruct((SLOTS, ROWS), bf16),
            jax.ShapeDtypeStruct(half, bf16),
        ),
        in_specs=[vmem] * 2 + [hbm] * 14,
        out_specs=(vmem,) * 3 + (hbm,),
        scratch_shapes=[
            pltpu.VMEM((SPAN, 256), bf16),
            pltpu.VMEM((2 * HD, SPAN), bf16),
            pltpu.VMEM((1024, D), bf16),
            pltpu.VMEM((ROWS, D), bf16),
            pltpu.VMEM((1, D), jnp.float32),
            pltpu.VMEM((1, D), jnp.float32),
            pltpu.VMEM((TOPK, ROWS), jnp.int32),
            pltpu.VMEM((TOPK, ROWS), jnp.float32),
            pltpu.SMEM((4,), jnp.float32),
            pltpu.VMEM((5, W, 128), bf16),
            pltpu.VMEM((5, 1, 128), jnp.int32),
            pltpu.VMEM((NT, ROWS, 256), bf16),
            pltpu.VMEM((NT, ROWS, 256), bf16),
            pltpu.VMEM((ROWS, D), bf16),
            pltpu.VMEM((SLOTS, ROWS), bf16),
            pltpu.VMEM(half, bf16),
            pltpu.VMEM((4, D, TILE), bf16),
            pltpu.VMEM((4, D, TILE), bf16),
            pltpu.VMEM((4, TILE, D), bf16),
            pltpu.VMEM((4, NCOL, CAP, D), bf16),
            pltpu.VMEM((NCOL, CAP, D), bf16),
            pltpu.VMEM((count, D), bf16),
            pltpu.VMEM((4, count, TILE), bf16),
            pltpu.VMEM((NCOL, CAP, D), bf16),
            pltpu.VMEM(third, bf16),
            pltpu.VMEM(third, bf16),
            pltpu.VMEM(half, bf16),
            dma((13,)),
            dma((2, 4)),
            dma((2, 4)),
            dma((2, 3, 2)),
            dma((2, 3, 2)),
            dma((2, NCOL)),
            dma((2, NCOL)),
            dma((2,)),
            dma((2, 3, len(SPLIT))),
            dma((2, 3, len(SPLIT))),
            dma((2, NCOL)),
            dma((2, NCOL)),
        ],
        compiler_params=pltpu.CompilerParams(
            collective_id=0, has_side_effects=True, vmem_limit_bytes=60 << 20
        ),
        cost_estimate=pl.CostEstimate(
            flops=14_000_000_000, bytes_accessed=300_000_000, transcendentals=0
        ),
    )(*arrays)


def rms_scale(vector):
    return vector * lax.rsqrt(jnp.mean(vector * vector, axis=-1, keepdims=True) + 1e-06)


def body(
    residual,
    queries,
    keys,
    values,
    documents,
    sink,
    out_weight,
    mix_gain,
    ffn_gain,
    out_gain,
    routes,
    route_logits,
    gate_weight,
    up_weight,
    down_weight,
):
    positions = lax.axis_index("sp") * SPAN + jnp.arange(SPAN, dtype=jnp.int32)
    half_size = HD // 2
    lanes = jnp.arange(128, dtype=jnp.int32)
    inverse = 10000.0 ** (-(lanes % half_size).astype(jnp.float32) / half_size)
    angles = positions.astype(jnp.float32)[:, None] * inverse[None, :]
    sign = jnp.where(lanes % HD < half_size, -1.0, 1.0)
    cosine, sine = jnp.cos(angles), jnp.sin(angles) * sign[None, :]
    after_mix, coarse, fine, returned = layer(
        cosine,
        sine,
        documents,
        sink,
        queries,
        keys.T,
        values.T,
        out_weight,
        residual,
        mix_gain.reshape(1, D),
        ffn_gain.reshape(1, D),
        routes.T,
        route_logits.T,
        gate_weight[0],
        up_weight[0],
        down_weight[0],
    )
    returned = returned.reshape(SLOTS, D)
    contract = (((0,), (0,)), ((), ()))
    expert_mix = lax.dot_general(
        coarse, returned, contract, preferred_element_type=jnp.float32
    ) + lax.dot_general(fine, returned, contract, preferred_element_type=jnp.float32)
    return (after_mix + rms_scale(expert_mix) * out_gain).astype(jnp.bfloat16)


def solution(mesh):
    in_specs = (
        P(("sp", "tp"), None),
        P("sp", "tp"),
        P("sp", "tp"),
        P("sp", "tp"),
        P("sp"),
        P("tp"),
        P(),
        P(),
        P(),
        P(),
        P(("sp", "tp"), None),
        P(("sp", "tp"), None),
        P("sp", None, "tp"),
        P("sp", None, "tp"),
        P("sp", "tp", None),
    )
    out_specs = P(("sp", "tp"), None)
    return jax.shard_map(body, mesh=mesh, in_specs=in_specs, out_specs=out_specs, check_vma=False)
```
